512 devices in a mesh: sp: 64 (over z, y), tp: 8 (over x, core).
Axes of the slice: x: 4, y: 8, z: 8, core: 2. Of those that a mesh axis runs over, the one named last changes fastest.
Arguments:
- block_input: bfloat16 [24576, 2048], P('sp'), may hold values from -16 to 16
- proj_x: bfloat16 [2048, 1024], P(None, 'tp'), may hold values from -0.125 to 0.125
- proj_gate: bfloat16 [2048, 1024], P(None, 'tp'), may hold values from -0.125 to 0.125
- conv_taps: float32 [4, 1024], P(None, 'tp'), may hold values from -3 to 3
- gate_a: bfloat16 [16, 64, 64], P('tp'), may hold values from -0.75 to 0.75
- gate_in: bfloat16 [16, 64, 64], P('tp'), may hold values from -0.75 to 0.75
- decay_param: float32 [1024], P('tp'), may hold values from 3 to 30
- log_jump: float32 [24576, 1024], P('sp', 'tp'), may hold values from -1 to 0, as said below
- out_grad: bfloat16 [24576, 1024], P('sp', 'tp'), may hold values from -6 to 6
Outputs:
- grad_input: bfloat16 [24576, 2048], P(('sp', 'tp'))
- grad_proj: float32 [2048, 1024], P('sp', 'tp')
The draws below stay inside these ranges and needn't reach their ends.
Inputs may be any that keep to these rules, and one draw needn't show every extreme that they name: `log_jump`: strictly negative.
All inputs are finite; a program needn't handle non-finite values.
Results may differ from the reference program's by a relative error of at most 0.015.
Values may be sent and summed in bfloat16 or wider, within the bound.
No kernel may reach another device: no remote copies, remote signals or barrier semaphores. Data moves between devices by JAX's collectives and lax.ppermute only.
A program may use at most 64 MiB of HBM per device.

```python
import math
import jax
import jax.numpy as jnp
from jax import lax

D = 2048
RECUR_CHANNELS = 1024
BLOCK = 64
TAPS = 4
TOK_DEV = 384
BLOCKS = 16
SEQUENCE_TOKENS = 24576
N_TP = 8


def draw_decay_param(key, part):
    key_kind = jax.random.fold_in(key, 11)
    key_fast = jax.random.fold_in(key, 12)
    key_slow = jax.random.fold_in(key, 13)
    fast_share = 0.5
    is_fast = jax.random.uniform(key_kind, (RECUR_CHANNELS,), jnp.float32) < fast_share
    fast_rate = jnp.exp(jax.random.uniform(key_fast, (RECUR_CHANNELS,), jnp.float32, math.log(1.0 / 400.0), math.log(1.0 / 120.0)))
    slow_rate = jax.random.uniform(key_slow, (RECUR_CHANNELS,), jnp.float32, 0.05, 0.3) * math.log(10.0) / (4.0 * SEQUENCE_TOKENS)
    rate = jnp.where(is_fast, fast_rate, slow_rate)
    return (-rate - jnp.log(-jnp.expm1(-rate))).astype(jnp.float32)


def draw_log_jump(key, part):
    key_block = jax.random.fold_in(key, 21)
    random_key_mask = jax.random.fold_in(key, 22)
    key_depth = jax.random.fold_in(key, 23)
    block_count = SEQUENCE_TOKENS // TOK_DEV
    spread = math.log(2.0)
    factor = jnp.exp(jax.random.uniform(key_block, (block_count, RECUR_CHANNELS), jnp.float32, -spread, spread))
    base_offset = -math.log(10.0) / (8.0 * SEQUENCE_TOKENS) * jnp.repeat(factor, TOK_DEV, axis=0)
    spike_mask = jax.random.uniform(random_key_mask, (SEQUENCE_TOKENS, RECUR_CHANNELS), jnp.float32) < 2.0 / SEQUENCE_TOKENS
    layer_depth = jnp.log(jax.random.uniform(key_depth, (SEQUENCE_TOKENS, RECUR_CHANNELS), jnp.float32, 0.55, 0.8))
    return (base_offset + jnp.where(spike_mask, layer_depth, 0.0)).astype(jnp.float32)


def spiked(drawn, own_key, source, target, parts, factor):
    owner, partner = [(jnp.arange(drawn.shape[dim]) // (drawn.shape[dim] // parts)).reshape([-1 if axis == dim else 1 for axis in range(drawn.ndim)]) for dim in (source, target)]
    chosen = jax.random.permutation(own_key, parts)[partner]
    strong = (owner == chosen) | (owner == (partner + parts // 2) % parts)
    return jnp.where(strong, factor * drawn, drawn)


def levels(stream_key, dims, pieces, smallest, high):
    gain = 1.0
    for axis_at, shards_of in pieces:
        steps = jax.random.uniform(jax.random.fold_in(jax.random.fold_in(stream_key, 6), axis_at), (shards_of,), jnp.float32, smallest / len(pieces), high / len(pieces))
        gain = gain * jnp.repeat(jnp.exp(steps), dims[axis_at] // shards_of).reshape((-1,) + (1,) * (len(dims) - 1 - axis_at))
    return gain


def centred(stream_key, shape, scale, bound, split=(), held_as=jnp.bfloat16):
    result = jax.random.normal(stream_key, shape, jnp.float32) * scale
    if len(split) > 0:
        result = levels(stream_key, shape, split, -0.22, 0.18) * result
    return jnp.clip(result, min=-bound, max=bound).astype(held_as)


def bell_draw_with(own_key, extent, scale, reach, split, heavy, held_as=jnp.bfloat16):
    array = scale * jax.random.normal(own_key, extent, jnp.float32)
    if split:
        array = array * levels(own_key, extent, split, -0.22, 0.18)
    return jnp.clip(spiked(array, jax.random.fold_in(own_key, 3), *heavy), -reach, reach).astype(held_as)


def setup_inputs(seed: int = 0) -> dict:
    key_of = jax.random.split(jax.random.key(seed), 10)
    block_input = bell_draw_with(key_of[0], (SEQUENCE_TOKENS, D), 1.0, 16.0, ((0, 64),), (0, 1, 64, 4.0))
    proj_x = centred(key_of[1], (D, RECUR_CHANNELS), D ** -0.5, 0.125, ((1, 8),))
    proj_gate = centred(key_of[2], (D, RECUR_CHANNELS), D ** -0.5, 0.125, ((1, 8),))
    conv_taps = centred(key_of[3], (TAPS, RECUR_CHANNELS), TAPS ** -0.5, 3.0, ((1, 8),), jnp.float32)
    gate_a = centred(key_of[4], (BLOCKS, BLOCK, BLOCK), BLOCK ** -0.5, 0.75, ((0, 8),))
    gate_in = centred(key_of[5], (BLOCKS, BLOCK, BLOCK), BLOCK ** -0.5, 0.75, ((0, 8),))
    decay_param = draw_decay_param(jax.random.fold_in(key_of[9], 71), 0)
    log_jump = draw_log_jump(jax.random.fold_in(key_of[9], 71), 0)
    out_grad = centred(key_of[8], (SEQUENCE_TOKENS, RECUR_CHANNELS), 1.0, 6.0, ((0, 64), (1, 8)))
    return {"block_input": block_input, "proj_x": proj_x, "proj_gate": proj_gate, "conv_taps": conv_taps, "gate_a": gate_a, "gate_in": gate_in, "decay_param": decay_param, "log_jump": log_jump, "out_grad": out_grad}


gate_power = 8.0

def combine(earlier, later):
    return (earlier[0] * later[0], later[0] * earlier[1] + later[1])

def reference(block_input, proj_x, proj_gate, conv_taps, gate_a, gate_in, decay_param, log_jump, out_grad):
    branch = jnp.dot(block_input, proj_x, preferred_element_type=jnp.float32).astype(jnp.bfloat16)
    gate_pre = jnp.dot(block_input, proj_gate, preferred_element_type=jnp.float32).astype(jnp.bfloat16)
    padded = jnp.pad(branch.astype(jnp.float32), ((TAPS - 1, 0), (0, 0)))
    mixed_sum = jnp.zeros((SEQUENCE_TOKENS, RECUR_CHANNELS), jnp.float32)
    for offset in range(TAPS):
        mixed_sum = mixed_sum + conv_taps[offset][None, :] * padded[offset:offset + SEQUENCE_TOKENS]
    mixed = mixed_sum.astype(jnp.bfloat16)
    mixed_f = mixed.astype(jnp.float32)
    mixed_blocks = mixed_f.reshape(SEQUENCE_TOKENS, BLOCKS, BLOCK)
    rec_gate = jax.nn.sigmoid(jnp.einsum('tbi,bij->tbj', mixed_blocks, gate_a.astype(jnp.float32)).reshape(SEQUENCE_TOKENS, RECUR_CHANNELS))
    in_gate = jax.nn.sigmoid(jnp.einsum('tbi,bij->tbj', mixed_blocks, gate_in.astype(jnp.float32)).reshape(SEQUENCE_TOKENS, RECUR_CHANNELS))
    log_sig = jax.nn.log_sigmoid(decay_param)
    log_decay = gate_power * rec_gate * log_sig[None, :] + log_jump
    decays = jnp.exp(log_decay)
    square_decay = jnp.exp(2.0 * log_decay)
    norm_factor = jnp.sqrt(-jnp.expm1(2.0 * log_decay))
    drive = norm_factor * in_gate * mixed_f
    _, hidden = lax.associative_scan(combine, (decays, drive), axis=0)
    activation, pullback = jax.vjp(jax.nn.gelu, gate_pre.astype(jnp.float32))
    grad_out = out_grad.astype(jnp.float32)
    grad_hidden = grad_out * activation
    next_decay = jnp.concatenate([decays[1:], jnp.ones((1, RECUR_CHANNELS), jnp.float32)], axis=0)
    _, flipped = lax.associative_scan(combine, (next_decay[::-1], grad_hidden[::-1]), axis=0)
    grad_state = flipped[::-1]
    hidden_prev = jnp.concatenate([jnp.zeros((1, RECUR_CHANNELS), jnp.float32), hidden[:-1]], axis=0)
    grad_log = grad_state * hidden_prev * decays - grad_state * in_gate * mixed_f * square_decay / norm_factor
    grad_pre_a = (grad_log * gate_power * log_sig[None, :] * rec_gate * (1.0 - rec_gate)).astype(jnp.bfloat16)
    grad_pre_in = (grad_state * norm_factor * mixed_f * in_gate * (1.0 - in_gate)).astype(jnp.bfloat16)
    back_a = jnp.einsum('tbj,bij->tbi', grad_pre_a.astype(jnp.float32).reshape(SEQUENCE_TOKENS, BLOCKS, BLOCK), gate_a.astype(jnp.float32))
    back_in = jnp.einsum('tbj,bij->tbi', grad_pre_in.astype(jnp.float32).reshape(SEQUENCE_TOKENS, BLOCKS, BLOCK), gate_in.astype(jnp.float32))
    grad_mixed = grad_state * norm_factor * in_gate + (back_a + back_in).reshape(SEQUENCE_TOKENS, RECUR_CHANNELS)
    padded_grad = jnp.pad(grad_mixed, ((0, TAPS - 1), (0, 0)))
    branch_sum = jnp.zeros((SEQUENCE_TOKENS, RECUR_CHANNELS), jnp.float32)
    for offset in range(TAPS):
        start = TAPS - 1 - offset
        branch_sum = branch_sum + conv_taps[offset][None, :] * padded_grad[start:start + SEQUENCE_TOKENS]
    grad_branch = branch_sum.astype(jnp.bfloat16)
    stored_hidden = lax.optimization_barrier(hidden.astype(jnp.bfloat16)).astype(jnp.float32)
    grad_gate = pullback(grad_out * stored_hidden)[0].astype(jnp.bfloat16)
    grad_proj = lax.dot_general(block_input, grad_branch, (((0,), (0,)), ((), ())), preferred_element_type=jnp.float32)
    group_width = RECUR_CHANNELS // N_TP
    total = jnp.zeros((SEQUENCE_TOKENS, D), jnp.float32)
    for group in range(N_TP):
        lower = group * group_width
        upper = lower + group_width
        partial_sum = lax.dot_general(grad_branch[:, lower:upper], proj_x[:, lower:upper], (((1,), (1,)), ((), ())), preferred_element_type=jnp.float32)
        partial_sum = partial_sum + lax.dot_general(grad_gate[:, lower:upper], proj_gate[:, lower:upper], (((1,), (1,)), ((), ())), preferred_element_type=jnp.float32)
        total = total + lax.optimization_barrier(partial_sum.astype(jnp.bfloat16)).astype(jnp.float32)
    return (total.astype(jnp.bfloat16), grad_proj)
```

```python
import jax
import jax.numpy as jnp
from jax import lax
from jax.experimental import pallas as pl
from jax.experimental.pallas import tpu as pltpu
from jax.sharding import Mesh
from jax.sharding import PartitionSpec as P

SP = ("sp_0", "sp_1")
SP_TP = ("sp_0", "sp_1", "tp_0", "tp_1")

GATE_POWER = 8.0
LANES = 128
SUB = 8
F32 = jnp.float32
BF16 = jnp.bfloat16
GELU_A = 0.7978845608028654
GELU_B = 0.044715


VMEM = pl.BlockSpec(memory_space=pltpu.VMEM)


def rounded(x):
    return x.astype(BF16).astype(F32)


def log_sigmoid(x):
    u = jnp.exp(-jnp.abs(x))
    series = u * (1.0 - u * (1 / 2 - u * (1 / 3 - u * (1 / 4 - u * (1 / 5 - u * (1 / 6 - u / 7))))))
    return jnp.minimum(x, 0.0) - jnp.where(u < 0.06, series, jnp.log(1.0 + u))


def one_minus_exp(x):
    near = jnp.maximum(x, -0.5)
    poly = 1.0 + near * (
        1 / 2
        + near
        * (
            1 / 6
            + near
            * (1 / 24 + near * (1 / 120 + near * (1 / 720 + near * (1 / 5040 + near / 40320))))
        )
    )
    return jnp.where(x > -0.5, -near * poly, 1.0 - jnp.exp(x))


def block_diagonal(pair_ref, into_ref, column):
    count, width = pair_ref.shape[0], pair_ref.shape[1]
    for b in range(count):
        at = column + b * width
        into_ref[b * width : (b + 1) * width, at : at + width] = pair_ref[b]


def fill_maps(a_ref, i_ref, map_ref):
    map_ref[...] = jnp.zeros(map_ref.shape, map_ref.dtype)
    block_diagonal(a_ref, map_ref, 0)
    block_diagonal(i_ref, map_ref, LANES)


def gates_of(ext_ref, rows, taps_ref, map_ref, param_ref, log_jump):
    lead = SUB - taps_ref.shape[0] + 1
    total = taps_ref[0:1, :] * ext_ref[lead : lead + rows, :]
    for j in range(1, taps_ref.shape[0]):
        total = total + taps_ref[j : j + 1, :] * ext_ref[lead + j : lead + j + rows, :]
    mixed = total.astype(BF16)
    both = jnp.dot(mixed, map_ref[...], preferred_element_type=F32)
    rec = jax.nn.sigmoid(both[:, :LANES])
    ing = jax.nn.sigmoid(both[:, LANES:])
    log_sig = log_sigmoid(param_ref[...])
    log_decay = GATE_POWER * rec * log_sig + log_jump
    decays = jnp.exp(log_decay)
    room = one_minus_exp(log_decay) * (1.0 + decays)
    return mixed.astype(F32), rec, ing, log_sig, decays, room


def gelu_parts(x):
    return jnp.tanh(GELU_A * (x + GELU_B * x * x * x))


def then(first, second):
    return first[0] * second[0], second[0] * first[1] + second[1]


def prefix_rows(a, f, backward):
    row = lax.broadcasted_iota(jnp.int32, a.shape, 0)
    for by in (1, 2, 4):
        shift = SUB - by if backward else by
        keep = row < SUB - by if backward else row >= by
        pa = jnp.where(keep, pltpu.roll(a, shift, 0), 1.0)
        pf = jnp.where(keep, pltpu.roll(f, shift, 0), 0.0)
        a, f = then((pa, pf), (a, f))
    return a, f


def exclusive_rows(a, f, backward):
    row = lax.broadcasted_iota(jnp.int32, a.shape, 0)
    a, f = prefix_rows(a, f, backward)
    shift = SUB - 1 if backward else 1
    keep = row < SUB - 1 if backward else row >= 1
    return (
        jnp.where(keep, pltpu.roll(a, shift, 0), 1.0),
        jnp.where(keep, pltpu.roll(f, shift, 0), 0.0),
    )


def project_kernel(x_ref, wx_ref, wg_ref, branch_ref, gate_ref, tail_ref, acc_ref):
    step = pl.program_id(0)
    both = jnp.concatenate([wx_ref[...], wg_ref[...]], axis=1)
    part = jnp.dot(x_ref[...], both, preferred_element_type=F32)

    @pl.when(step == 0)
    def _():
        acc_ref[...] = part

    @pl.when(step > 0)
    def _():
        acc_ref[...] += part

    @pl.when(step == pl.num_programs(0) - 1)
    def _():
        branch = rounded(acc_ref[:, :LANES])
        branch_ref[...] = branch
        gate_ref[...] = rounded(acc_ref[:, LANES:])
        tail_ref[...] = branch[branch.shape[0] - SUB :]


def project(block_input, proj_x, proj_gate):
    rows, width = block_input.shape
    steps = 4 if width % (4 * LANES) == 0 else 1
    deep = width // steps
    return pl.pallas_call(
        project_kernel,
        grid=(steps,),
        in_specs=[
            pl.BlockSpec((rows, deep), lambda k: (0, k)),
            pl.BlockSpec((deep, LANES), lambda k: (k, 0)),
            pl.BlockSpec((deep, LANES), lambda k: (k, 0)),
        ],
        out_specs=[
            pl.BlockSpec((rows, LANES), lambda k: (0, 0)),
            pl.BlockSpec((rows, LANES), lambda k: (0, 0)),
            pl.BlockSpec((SUB, LANES), lambda k: (0, 0)),
        ],
        out_shape=[
            jax.ShapeDtypeStruct((rows, LANES), F32),
            jax.ShapeDtypeStruct((rows, LANES), F32),
            jax.ShapeDtypeStruct((SUB, LANES), F32),
        ],
        scratch_shapes=[pltpu.VMEM((rows, 2 * LANES), F32)],
        cost_estimate=pl.CostEstimate(
            flops=4 * rows * width * LANES, bytes_accessed=4 * width * (rows + LANES), transcendentals=0
        ),
        name="project",
    )(block_input, proj_x, proj_gate)


def summary_kernel(
    before_ref, branch_ref, gate_ref, out_grad_ref, jump_ref, taps_ref, a_ref, i_ref, param_ref,
    sent_ref, head_ref, ext_ref, map_ref, d_ref, x_ref, g_ref,
):
    rows = branch_ref.shape[0]
    edge = taps_ref.shape[0] - 1
    ext_ref[0:SUB, :] = before_ref[...]
    ext_ref[SUB : SUB + rows, :] = branch_ref[...]
    fill_maps(a_ref, i_ref, map_ref)
    mixed, _, ing, _, decays, room = gates_of(
        ext_ref, rows, taps_ref, map_ref, param_ref, jump_ref[...]
    )
    d_ref[...] = decays
    x_ref[...] = jnp.sqrt(room) * ing * mixed
    gate = gate_ref[...]
    g_ref[...] = out_grad_ref[...].astype(F32) * (0.5 * gate * (1.0 + gelu_parts(gate)))

    head_ref[...] = jnp.zeros(head_ref.shape, F32)
    head_ref[0:edge, :] = branch_ref[0:edge, :]
    head_ref[edge : 2 * edge, :] = jump_ref[0:edge, :]
    head_ref[2 * edge : 3 * edge, :] = g_ref[0:edge, :]

    long = rows // SUB
    row = lax.broadcasted_iota(jnp.int32, (SUB, LANES), 0)
    decay = [d_ref[pl.ds(i, SUB, stride=long), :] for i in range(long)]
    fa, ff = decay[0], x_ref[pl.ds(0, SUB, stride=long), :]
    for i in range(1, long):
        fa, ff = then((fa, ff), (decay[i], x_ref[pl.ds(i, SUB, stride=long), :]))
    ba = jnp.ones((SUB, LANES), F32)
    bf = jnp.zeros((SUB, LANES), F32)
    for i in range(long - 1, -1, -1):
        na = ba * decay[i]
        nf = decay[i] * (g_ref[pl.ds(i, SUB, stride=long), :] + bf)
        ba, bf = (jnp.where(row == 0, ba, na), jnp.where(row == 0, bf, nf)) if i < edge else (na, nf)
    _, f_all = prefix_rows(fa, ff, False)
    b_all, r_all = prefix_rows(ba, bf, True)
    late_a, late_r = b_all[0:1, :], r_all[0:1, :]
    head_ref[3 * edge : 3 * edge + 1, :] = late_a
    head_ref[3 * edge + 1 : 3 * edge + 2, :] = late_r
    whole_a, whole_r = late_a, late_r
    for t in range(edge - 1, -1, -1):
        d = d_ref[t : t + 1, :]
        whole_a = whole_a * d
        whole_r = d * (g_ref[t : t + 1, :] + whole_r)
    lines = jnp.where(
        row % 4 == 0, whole_a, jnp.where(row % 4 == 1, f_all[SUB - 1 : SUB, :], whole_r)
    )
    for k in range(sent_ref.shape[0] // SUB):
        sent_ref[k * SUB : (k + 1) * SUB, :] = lines


def summary(before, branch, gate, out_grad, jump, taps, a, i, param, peers):
    rows = branch.shape[0]
    return pl.pallas_call(
        summary_kernel,
        in_specs=[VMEM] * 9,
        out_specs=[VMEM] * 2,
        out_shape=[
            jax.ShapeDtypeStruct((peers * 4, LANES), F32),
            jax.ShapeDtypeStruct((2 * SUB, LANES), F32),
        ],
        scratch_shapes=[
            pltpu.VMEM((rows + SUB, LANES), F32),
            pltpu.VMEM((LANES, 2 * LANES), BF16),
            pltpu.VMEM((rows, LANES), F32),
            pltpu.VMEM((rows, LANES), F32),
            pltpu.VMEM((rows, LANES), F32),
        ],
        cost_estimate=pl.CostEstimate(flops=rows * 200000, bytes_accessed=rows * 2048, transcendentals=0),
        name="summary",
    )(before, branch, gate, out_grad, jump, taps, a, i, param)


def prepare_kernel(
    before_ref, after_ref, branch_ref, gate_ref, out_grad_ref, jump_ref, taps_ref, a_ref, i_ref, param_ref,
    d_ref, x_ref, g_ref, p1_ref, p2_ref, p3_ref, p4_ref, q_ref, seg_ref, ext_ref, map_ref, jump_ext, nat_ref,
):
    rows = branch_ref.shape[0]
    full = rows + SUB
    edge = taps_ref.shape[0] - 1
    long = full // SUB
    ext_ref[0:SUB, :] = before_ref[...]
    ext_ref[SUB : SUB + rows, :] = branch_ref[...]
    ext_ref[SUB + rows :, :] = jnp.zeros((SUB, LANES), F32)
    ext_ref[SUB + rows : SUB + rows + edge, :] = after_ref[0:edge, :]
    jump_ext[0:rows, :] = jump_ref[...]
    jump_ext[rows:, :] = jnp.full((SUB, LANES), -1.0, F32)
    near = after_ref[edge : 2 * edge, :]
    jump_ext[rows : rows + edge, :] = jnp.where(near < 0.0, near, -1.0)
    fill_maps(a_ref, i_ref, map_ref)
    mixed, rec, ing, log_sig, decays, room = gates_of(
        ext_ref, full, taps_ref, map_ref, param_ref, jump_ext[...]
    )
    inverse = lax.rsqrt(room)
    norm = room * inverse
    real = lax.broadcasted_iota(jnp.int32, (full, LANES), 0) < rows + edge

    def put(value, into):
        nat_ref[...] = value
        for i in range(long):
            into[i * SUB : (i + 1) * SUB, :] = nat_ref[pl.ds(i, SUB, stride=long), :]

    swing = GATE_POWER * log_sig * rec * (1.0 - rec)
    put(jnp.where(real, decays, 1.0), d_ref)
    put(norm * ing * mixed, x_ref)
    put(decays * swing, p1_ref)
    put(ing * mixed * decays * decays * inverse * swing, p2_ref)
    put(norm * mixed * ing * (1.0 - ing), p3_ref)
    put(norm * ing, p4_ref)
    gate = gate_ref[...]
    t = gelu_parts(gate)
    grad = out_grad_ref[...].astype(F32)
    nat_ref[rows:, :] = jnp.zeros((SUB, LANES), F32)
    nat_ref[0:rows, :] = grad * (
        0.5 * (1.0 + t) + 0.5 * gate * (1.0 - t * t) * GELU_A * (1.0 + 3.0 * GELU_B * gate * gate)
    )
    for i in range(long):
        q_ref[i * SUB : (i + 1) * SUB, :] = nat_ref[pl.ds(i, SUB, stride=long), :]
    nat_ref[0:rows, :] = grad * (0.5 * gate * (1.0 + t))
    nat_ref[rows : rows + edge, :] = after_ref[2 * edge : 3 * edge, :]
    for i in range(long):
        g_ref[i * SUB : (i + 1) * SUB, :] = nat_ref[pl.ds(i, SUB, stride=long), :]

    at = lambda ref, i: ref[i * SUB : (i + 1) * SUB, :]
    fa, ff = at(d_ref, 0), at(x_ref, 0)
    for i in range(1, long):
        fa, ff = then((fa, ff), (at(d_ref, i), at(x_ref, i)))
    bf = jnp.zeros((SUB, LANES), F32)
    for i in range(long - 1, -1, -1):
        bf = at(d_ref, i) * (at(g_ref, i) + bf)
    ea, ef = exclusive_rows(fa, ff, False)
    ra, rf = exclusive_rows(fa, bf, True)
    for k, value in enumerate((ea, ef, ra, rf)):
        seg_ref[k * SUB : (k + 1) * SUB, :] = value


def prepare(before, after, branch, gate, out_grad, jump, taps, a, i, param):
    rows = branch.shape[0]
    full = rows + SUB
    return pl.pallas_call(
        prepare_kernel,
        in_specs=[VMEM] * 10,
        out_specs=[VMEM] * 9,
        out_shape=[jax.ShapeDtypeStruct((full, LANES), F32)] * 8
        + [jax.ShapeDtypeStruct((4 * SUB, LANES), F32)],
        scratch_shapes=[
            pltpu.VMEM((full + SUB, LANES), F32),
            pltpu.VMEM((LANES, 2 * LANES), BF16),
            pltpu.VMEM((full, LANES), F32),
            pltpu.VMEM((full, LANES), F32),
        ],
        cost_estimate=pl.CostEstimate(flops=rows * 400000, bytes_accessed=rows * 8192, transcendentals=0),
        name="prepare",
    )(before, after, branch, gate, out_grad, jump, taps, a, i, param)


def finish_kernel(
    place_ref, all_ref, after_ref, d_ref, x_ref, g_ref, p1_ref, p2_ref, p3_ref, p4_ref, q_ref, seg_ref,
    taps_ref, a_ref, i_ref, gb_ref, gg_ref, map_ref, pre_ref, gm_ref, nat_ref, nat2_ref,
):
    edge = taps_ref.shape[0] - 1
    full = d_ref.shape[0]
    rows = full - SUB
    long = full // SUB
    me = place_ref[0]
    peers = all_ref.shape[0] // 4
    each = peers // SUB
    row = lax.broadcasted_iota(jnp.int32, (SUB, LANES), 0)
    fill_maps(a_ref, i_ref, map_ref)
    ones, zeros = jnp.ones((SUB, LANES), F32), jnp.zeros((SUB, LANES), F32)

    def line(i, q):
        return all_ref[pl.ds(4 * i + q, SUB, stride=4 * each), :]

    fwd, bwd = (ones, zeros), (ones, zeros)
    for i in range(each):
        k = row * each + i
        fwd = then(fwd, (jnp.where(k < me, line(i, 0), 1.0), jnp.where(k < me, line(i, 1), 0.0)))
        o = each - 1 - i
        k = row * each + o
        bwd = then(
            bwd, (jnp.where(k > me + 1, line(o, 0), 1.0), jnp.where(k > me + 1, line(o, 2), 0.0))
        )
    state_in = prefix_rows(*fwd, False)[1][SUB - 1 : SUB, :]
    beyond = prefix_rows(*bwd, True)[1][0:1, :]
    carry_in = after_ref[3 * edge + 1 : 3 * edge + 2, :] + beyond * after_ref[3 * edge : 3 * edge + 1, :]

    part = lambda k: seg_ref[k * SUB : (k + 1) * SUB, :]
    at = lambda ref, i: ref[i * SUB : (i + 1) * SUB, :]
    carry = part(2) * carry_in + part(3)
    for i in range(long - 1, -1, -1):
        gs = at(g_ref, i) + carry
        carry = at(d_ref, i) * gs
        gm_ref[i * SUB : (i + 1) * SUB, :] = gs
    hidden = part(0) * state_in + part(1)
    for i in range(long):
        gs = at(gm_ref, i)
        pre_a = gs * (hidden * at(p1_ref, i) - at(p2_ref, i))
        pre_i = gs * at(p3_ref, i)
        pre_ref[i * SUB : (i + 1) * SUB, 0:LANES] = pre_a
        pre_ref[i * SUB : (i + 1) * SUB, LANES:] = pre_i
        hidden = at(d_ref, i) * hidden + at(x_ref, i)
        nat_ref[pl.ds(i, SUB, stride=long), :] = rounded(hidden) * at(q_ref, i)
    gg_ref[...] = nat_ref[0:rows, :].astype(BF16)
    back = lax.dot_general(
        pre_ref[...].astype(BF16), map_ref[...], (((1,), (1,)), ((), ())), preferred_element_type=F32
    )
    gm_ref[...] = gm_ref[...] * p4_ref[...] + back
    turned = [pltpu.roll(at(gm_ref, i), SUB - 1, 0) for i in range(edge)]
    for i in range(long):
        total = None
        for j in range(edge + 1):
            k = i + edge - j
            term = taps_ref[j : j + 1, :] * (at(gm_ref, k) if k < long else turned[k - long])
            total = term if total is None else total + term
        nat2_ref[pl.ds(i, SUB, stride=long), :] = total
    gb_ref[...] = nat2_ref[0:rows, :].astype(BF16)


def finish(place, every, after, d, x, g, p1, p2, p3, p4, q, seg, taps, a, i):
    full = d.shape[0]
    rows = full - SUB
    return pl.pallas_call(
        finish_kernel,
        in_specs=[pl.BlockSpec(memory_space=pltpu.SMEM)] + [VMEM] * 14,
        out_specs=[VMEM] * 2,
        out_shape=[jax.ShapeDtypeStruct((rows, LANES), BF16)] * 2,
        scratch_shapes=[
            pltpu.VMEM((LANES, 2 * LANES), BF16),
            pltpu.VMEM((full, 2 * LANES), F32),
            pltpu.VMEM((full, LANES), F32),
            pltpu.VMEM((full, LANES), F32),
            pltpu.VMEM((full, LANES), F32),
        ],
        cost_estimate=pl.CostEstimate(flops=rows * 400000, bytes_accessed=rows * 8192, transcendentals=0),
        name="finish",
    )(place, every, after, d, x, g, p1, p2, p3, p4, q, seg, taps, a, i)


def shifted(x, axis, by):
    count = lax.axis_size(axis)
    return lax.ppermute(x, axis, [(i, i + by) for i in range(count) if 0 <= i + by < count])


def body(
    block_input, proj_x, proj_gate, conv_taps, gate_a, gate_in, decay_param, log_jump, out_grad
):
    peers = lax.axis_size(SP)
    chips = lax.axis_size("tp_0")
    rows = block_input.shape[0]
    place = lax.axis_index(SP).astype(jnp.int32).reshape(1)
    chip, core = lax.axis_index("tp_0"), lax.axis_index("tp_1")
    param = decay_param.reshape(1, LANES)
    swap = [(0, 1), (1, 0)]

    mine = jnp.concatenate([proj_x, proj_gate], axis=1)
    theirs = lax.ppermute(mine, "tp_1", swap)

    branch, gate, tail = project(block_input, proj_x, proj_gate)
    before = shifted(tail, SP, 1)
    sent, head = summary(
        before, branch, gate, out_grad, log_jump, conv_taps, gate_a, gate_in, param, peers
    )
    every = lax.all_to_all(sent, SP, 0, 0, tiled=True)
    after = shifted(head, SP, -1)
    parts = prepare(
        before, after, branch, gate, out_grad, log_jump, conv_taps, gate_a, gate_in, param
    )
    grad_branch, grad_gate = finish(place, every, after, *parts, conv_taps, gate_a, gate_in)

    grads = jnp.concatenate([grad_branch, grad_gate], axis=1)
    cut = grads.reshape(chips, 2, rows // (2 * chips), 2 * LANES)
    own = lax.dynamic_index_in_dim(cut, core, 1, keepdims=False)
    other = lax.dynamic_index_in_dim(cut, 1 - core, 1, keepdims=False)
    got = lax.ppermute(other, "tp_1", swap)

    partial = lax.dot_general(
        block_input, grad_branch, (((0,), (0,)), ((), ())), preferred_element_type=F32
    ).astype(BF16)
    pieces = lax.all_to_all(partial, SP, 0, 0, tiled=True)

    nt = (((2,), (1,)), ((), ()))
    mixed = lax.dot_general(own, mine, nt, preferred_element_type=F32) + lax.dot_general(
        got, theirs, nt, preferred_element_type=F32
    )
    mixed = mixed.astype(BF16)
    total = lax.dynamic_index_in_dim(mixed, chip, 0, keepdims=False).astype(F32)
    for by in range(1, chips):
        piece = lax.dynamic_index_in_dim(mixed, (chip + by) % chips, 0, keepdims=False)
        arrived = lax.ppermute(piece, "tp_0", [(k, (k + by) % chips) for k in range(chips)])
        total = total + arrived.astype(F32)
    grad_proj = jnp.sum(
        pieces.reshape(peers, partial.shape[0] // peers, LANES).astype(F32), axis=0
    )
    return total.astype(BF16), grad_proj


def solution(mesh):
    count = mesh.devices.size
    tp = mesh.shape["tp"]
    sp = count // tp
    first = next(k for k in (8, 4, 2, 1) if sp % k == 0 and sp // k >= k)
    split = Mesh(mesh.devices.reshape(first, sp // first, tp // 2, 2), SP_TP)
    tp_axes = ("tp_0", "tp_1")
    in_specs = (
        P(SP, None),
        P(None, tp_axes),
        P(None, tp_axes),
        P(None, tp_axes),
        P(tp_axes, None, None),
        P(tp_axes, None, None),
        P(tp_axes),
        P(SP, tp_axes),
        P(SP, tp_axes),
    )
    out_specs = (P(SP_TP, None), P(SP, tp_axes))
    return jax.shard_map(body, mesh=split, in_specs=in_specs, out_specs=out_specs, check_vma=False)
```

```python
import jax
import jax.numpy as jnp
from jax import lax
from jax.experimental import pallas as pl
from jax.experimental.pallas import tpu as pltpu
from jax.sharding import Mesh
from jax.sharding import PartitionSpec as P

SP = ("sp_0", "sp_1")
SP_TP = ("sp_0", "sp_1", "tp_0", "tp_1")

GATE_POWER = 8.0
LANES = 128
SUB = 8
F32 = jnp.float32
BF16 = jnp.bfloat16
GELU_A = 0.7978845608028654
GELU_B = 0.044715


VMEM = pl.BlockSpec(memory_space=pltpu.VMEM)


def rounded(x):
    return x.astype(BF16).astype(F32)


def log_sigmoid(x):
    u = jnp.exp(-jnp.abs(x))
    series = u * (1.0 - u * (1 / 2 - u * (1 / 3 - u * (1 / 4 - u * (1 / 5 - u * (1 / 6 - u / 7))))))
    return jnp.minimum(x, 0.0) - jnp.where(u < 0.06, series, jnp.log(1.0 + u))


def one_minus_exp(x):
    near = jnp.maximum(x, -0.5)
    poly = 1.0 + near * (
        1 / 2
        + near
        * (
            1 / 6
            + near
            * (1 / 24 + near * (1 / 120 + near * (1 / 720 + near * (1 / 5040 + near / 40320))))
        )
    )
    return jnp.where(x > -0.5, -near * poly, 1.0 - jnp.exp(x))


def block_diagonal(pair_ref, into_ref, column):
    count, width = pair_ref.shape[0], pair_ref.shape[1]
    for b in range(count):
        at = column + b * width
        into_ref[b * width : (b + 1) * width, at : at + width] = pair_ref[b]


def fill_maps(a_ref, i_ref, map_ref):
    map_ref[...] = jnp.zeros(map_ref.shape, map_ref.dtype)
    block_diagonal(a_ref, map_ref, 0)
    block_diagonal(i_ref, map_ref, LANES)


def gates_of(ext_ref, rows, taps_ref, map_ref, param_ref, log_jump):
    lead = SUB - taps_ref.shape[0] + 1
    total = taps_ref[0:1, :] * ext_ref[lead : lead + rows, :]
    for j in range(1, taps_ref.shape[0]):
        total = total + taps_ref[j : j + 1, :] * ext_ref[lead + j : lead + j + rows, :]
    mixed = total.astype(BF16)
    both = jnp.dot(mixed, map_ref[...], preferred_element_type=F32)
    rec = jax.nn.sigmoid(both[:, :LANES])
    ing = jax.nn.sigmoid(both[:, LANES:])
    log_sig = log_sigmoid(param_ref[...])
    log_decay = GATE_POWER * rec * log_sig + log_jump
    decays = jnp.exp(log_decay)
    room = one_minus_exp(log_decay) * (1.0 + decays)
    return mixed.astype(F32), rec, ing, log_sig, decays, room


def gelu_parts(x):
    return jnp.tanh(GELU_A * (x + GELU_B * x * x * x))


def then(first, second):
    return first[0] * second[0], second[0] * first[1] + second[1]


def prefix_rows(a, f, backward):
    row = lax.broadcasted_iota(jnp.int32, a.shape, 0)
    for by in (1, 2, 4):
        shift = SUB - by if backward else by
        keep = row < SUB - by if backward else row >= by
        pa = jnp.where(keep, pltpu.roll(a, shift, 0), 1.0)
        pf = jnp.where(keep, pltpu.roll(f, shift, 0), 0.0)
        a, f = then((pa, pf), (a, f))
    return a, f


def exclusive_rows(a, f, backward):
    row = lax.broadcasted_iota(jnp.int32, a.shape, 0)
    a, f = prefix_rows(a, f, backward)
    shift = SUB - 1 if backward else 1
    keep = row < SUB - 1 if backward else row >= 1
    return (
        jnp.where(keep, pltpu.roll(a, shift, 0), 1.0),
        jnp.where(keep, pltpu.roll(f, shift, 0), 0.0),
    )


def limits(mib):
    return pltpu.CompilerParams(vmem_limit_bytes=mib * 2**20)


def project_kernel(x_ref, wx_ref, wg_ref, branch_ref, gate_ref, tail_ref, x_in, w_in, acc_ref, sems):
    steps = sems.shape[0] // 3
    deep = x_in.shape[1] // steps
    copies = []
    for k in range(steps):
        at = slice(k * deep, (k + 1) * deep)
        trio = (
            (wx_ref.at[at, :], w_in.at[at, 0:LANES]),
            (wg_ref.at[at, :], w_in.at[at, LANES : 2 * LANES]),
            (x_ref.at[:, at], x_in.at[:, at]),
        )
        copies.append(
            [pltpu.make_async_copy(*pair, sems.at[3 * k + n]) for n, pair in enumerate(trio)]
        )
        for copy in copies[-1]:
            copy.start()
    for k in range(steps):
        for copy in copies[k]:
            copy.wait()
        at = slice(k * deep, (k + 1) * deep)
        part = jnp.dot(x_in[:, at], w_in[at, :], preferred_element_type=F32)
        acc_ref[...] = part if k == 0 else acc_ref[...] + part
    branch = rounded(acc_ref[:, :LANES])
    branch_ref[...] = branch
    gate_ref[...] = rounded(acc_ref[:, LANES:])
    tail_ref[...] = branch[branch.shape[0] - SUB :]


def project(block_input, proj_x, proj_gate):
    rows, width = block_input.shape
    steps = 4 if width % (4 * LANES) == 0 else 1
    hbm = pl.BlockSpec(memory_space=pltpu.HBM)
    return pl.pallas_call(
        project_kernel,
        in_specs=[hbm] * 3,
        out_specs=[VMEM] * 3,
        out_shape=[
            jax.ShapeDtypeStruct((rows, LANES), F32),
            jax.ShapeDtypeStruct((rows, LANES), F32),
            jax.ShapeDtypeStruct((SUB, LANES), F32),
        ],
        scratch_shapes=[
            pltpu.VMEM((rows, width), BF16),
            pltpu.VMEM((width, 2 * LANES), BF16),
            pltpu.VMEM((rows, 2 * LANES), F32),
            pltpu.SemaphoreType.DMA((3 * steps,)),
        ],
        cost_estimate=pl.CostEstimate(
            flops=4 * rows * width * LANES, bytes_accessed=4 * width * (rows + LANES), transcendentals=0
        ),
        compiler_params=limits(12),
        name="project",
    )(*(pltpu.with_memory_space_constraint(v, pltpu.HBM) for v in (block_input, proj_x, proj_gate)))


def factors(mixed, rec, ing, log_sig, decays, room):
    inverse = lax.rsqrt(room)
    norm = room * inverse
    swing = GATE_POWER * log_sig * rec * (1.0 - rec)
    pull = ing * mixed
    return (
        decays,
        norm * pull,
        decays * swing,
        pull * decays * decays * inverse * swing,
        norm * pull * (1.0 - ing),
        norm * ing,
    )


def row_of(ref, i):
    return ref[i * SUB : (i + 1) * SUB, :]


def sublanes():
    return lax.broadcasted_iota(jnp.int32, (SUB, LANES), 0)


def local_kernel(
    branch_ref, gate_ref, out_grad_ref, jump_ref, taps_ref, a_ref, i_ref, param_ref,
    d_ref, x_ref, p1_ref, p2_ref, p3_ref, p4_ref, g_ref, q_ref, misc_ref, ext_ref, map_ref, *nat_refs,
):
    rows = branch_ref.shape[0]
    long = rows // SUB
    ext_ref[0:SUB, :] = jnp.zeros((SUB, LANES), F32)
    ext_ref[SUB:, :] = branch_ref[...]
    fill_maps(a_ref, i_ref, map_ref)
    values = factors(*gates_of(ext_ref, rows, taps_ref, map_ref, param_ref, jump_ref[...]))
    gate = gate_ref[...]
    t = gelu_parts(gate)
    grad = out_grad_ref[...].astype(F32)
    g = grad * (0.5 * gate * (1.0 + t))
    q = grad * (
        0.5 * (1.0 + t) + 0.5 * gate * (1.0 - t * t) * GELU_A * (1.0 + 3.0 * GELU_B * gate * gate)
    )
    into = (d_ref, x_ref, p1_ref, p2_ref, p3_ref, p4_ref, g_ref, q_ref)
    for value, nat in zip((*values, g, q), nat_refs):
        nat[...] = value
    for nat, ref in zip(nat_refs, into):
        for i in range(long):
            ref[i * SUB : (i + 1) * SUB, :] = nat[pl.ds(i, SUB, stride=long), :]
    row = sublanes()
    ones, zeros = jnp.ones((SUB, LANES), F32), jnp.zeros((SUB, LANES), F32)
    fwd, bwd = (ones, zeros), (ones, zeros)
    for i in range(long):
        a, f = row_of(d_ref, i), row_of(x_ref, i)
        if i < SUB:
            a, f = jnp.where(row == 0, 1.0, a), jnp.where(row == 0, 0.0, f)
        fwd = then(fwd, (a, f))
        o = long - 1 - i
        a = row_of(d_ref, o)
        f = a * row_of(g_ref, o)
        if o < SUB:
            a, f = jnp.where(row == 0, 1.0, a), jnp.where(row == 0, 0.0, f)
        bwd = then(bwd, (a, f))
    fa, ff = prefix_rows(*fwd, False)
    ba, bf = prefix_rows(*bwd, True)
    misc_ref[0:1, :] = fa[SUB - 1 : SUB, :]
    misc_ref[1:2, :] = ff[SUB - 1 : SUB, :]
    misc_ref[2:3, :] = ba[0:1, :]
    misc_ref[3:4, :] = bf[0:1, :]
    misc_ref[4:SUB, :] = jnp.zeros((SUB - 4, LANES), F32)
    misc_ref[SUB:, :] = nat_refs[6][0:SUB, :]


def local(branch, gate, out_grad, jump, taps, a, i, param):
    rows = branch.shape[0]
    return pl.pallas_call(
        local_kernel,
        in_specs=[VMEM] * 8,
        out_specs=[VMEM] * 9,
        out_shape=[jax.ShapeDtypeStruct((rows, LANES), F32)] * 8
        + [jax.ShapeDtypeStruct((2 * SUB, LANES), F32)],
        scratch_shapes=[
            pltpu.VMEM((rows + SUB, LANES), F32),
            pltpu.VMEM((LANES, 2 * LANES), BF16),
        ]
        + [pltpu.VMEM((rows, LANES), F32)] * 8,
        cost_estimate=pl.CostEstimate(flops=rows * 300000, bytes_accessed=rows * 8192, transcendentals=0),
        compiler_params=limits(12),
        name="local",
    )(branch, gate, out_grad, jump, taps, a, i, param)


def summary_kernel(
    before_ref, branch_ref, jump_ref, taps_ref, a_ref, i_ref, param_ref, misc_ref,
    sent_ref, head_ref, patch_ref, ext_ref, map_ref,
):
    edge = taps_ref.shape[0] - 1
    ext_ref[0:SUB, :] = before_ref[...]
    ext_ref[SUB : 2 * SUB, :] = branch_ref[0:SUB, :]
    ext_ref[2 * SUB :, :] = jnp.zeros((SUB, LANES), F32)
    fill_maps(a_ref, i_ref, map_ref)
    values = factors(*gates_of(ext_ref, SUB, taps_ref, map_ref, param_ref, jump_ref[0:SUB, :]))
    for k, value in enumerate(values):
        patch_ref[k * SUB : (k + 1) * SUB, :] = value
    d, x = values[0], values[1]
    g = misc_ref[SUB:, :]
    fa, ff = prefix_rows(d, x, False)
    ba, bf = prefix_rows(d, d * g, True)
    whole = then(
        (fa[SUB - 1 : SUB, :], ff[SUB - 1 : SUB, :]), (misc_ref[0:1, :], misc_ref[1:2, :])
    )
    rest = misc_ref[2:3, :], misc_ref[3:4, :]
    late = then(rest, (ba[edge : edge + 1, :], bf[edge : edge + 1, :]))
    back = then(rest, (ba[0:1, :], bf[0:1, :]))
    head_ref[...] = jnp.zeros(head_ref.shape, F32)
    head_ref[0:edge, :] = branch_ref[0:edge, :]
    head_ref[edge : 2 * edge, :] = jump_ref[0:edge, :]
    head_ref[2 * edge : 3 * edge, :] = misc_ref[SUB : SUB + edge, :]
    head_ref[3 * edge : 3 * edge + 1, :] = late[0]
    head_ref[3 * edge + 1 : 3 * edge + 2, :] = late[1]
    row = sublanes()
    lines = jnp.where(row % 4 == 0, whole[0], jnp.where(row % 4 == 1, whole[1], back[1]))
    for k in range(sent_ref.shape[0] // SUB):
        sent_ref[k * SUB : (k + 1) * SUB, :] = lines


def summary(before, branch, jump, taps, a, i, param, misc, peers):
    return pl.pallas_call(
        summary_kernel,
        in_specs=[VMEM] * 8,
        out_specs=[VMEM] * 3,
        out_shape=[
            jax.ShapeDtypeStruct((peers * 4, LANES), F32),
            jax.ShapeDtypeStruct((2 * SUB, LANES), F32),
            jax.ShapeDtypeStruct((6 * SUB, LANES), F32),
        ],
        scratch_shapes=[
            pltpu.VMEM((3 * SUB, LANES), F32),
            pltpu.VMEM((LANES, 2 * LANES), BF16),
        ],
        cost_estimate=pl.CostEstimate(flops=10000000, bytes_accessed=1000000, transcendentals=0),
        compiler_params=limits(8),
        name="summary",
    )(before, branch, jump, taps, a, i, param, misc)


def patched(ref, patch_ref, k, i, row):
    if i >= SUB:
        return row_of(ref, i)
    at = k * SUB + i
    return jnp.where(row == 0, patch_ref[at : at + 1, :], row_of(ref, i))


def segments_kernel(d_ref, x_ref, g_ref, patch_ref, seg_ref):
    long = d_ref.shape[0] // SUB
    row = sublanes()
    fa, ff = jnp.ones((SUB, LANES), F32), jnp.zeros((SUB, LANES), F32)
    bf = ff
    for i in range(long):
        fa, ff = then((fa, ff), (patched(d_ref, patch_ref, 0, i, row), patched(x_ref, patch_ref, 1, i, row)))
        o = long - 1 - i
        bf = patched(d_ref, patch_ref, 0, o, row) * (row_of(g_ref, o) + bf)
    ea, ef = exclusive_rows(fa, ff, False)
    ra, rf = exclusive_rows(fa, bf, True)
    for k, value in enumerate((ea, ef, ra, rf)):
        seg_ref[k * SUB : (k + 1) * SUB, :] = value


def segments(d, x, g, patch):
    return pl.pallas_call(
        segments_kernel,
        in_specs=[VMEM] * 4,
        out_specs=VMEM,
        out_shape=jax.ShapeDtypeStruct((4 * SUB, LANES), F32),
        cost_estimate=pl.CostEstimate(flops=50000000, bytes_accessed=1000000, transcendentals=0),
        compiler_params=limits(8),
        name="segments",
    )(d, x, g, patch)


def finish_kernel(
    place_ref, all_ref, after_ref, d_ref, x_ref, p1_ref, p2_ref, p3_ref, p4_ref, g_ref, q_ref, patch_ref, seg_ref,
    branch_ref, taps_ref, a_ref, i_ref, param_ref, input_ref,
    gb_ref, gg_ref, gp_ref, map_ref, pre_ref, gm_ref, nat_ref, ext_ref, few_ref, input_in, sem,
):
    fetch = pltpu.make_async_copy(input_ref, input_in, sem)
    fetch.start()
    edge = taps_ref.shape[0] - 1
    rows = d_ref.shape[0]
    long = rows // SUB
    me = place_ref[0]
    peers = all_ref.shape[0] // 4
    each = peers // SUB
    row = sublanes()

    def own(ref, k, i):
        return patched(ref, patch_ref, k, i, row)

    fill_maps(a_ref, i_ref, map_ref)
    ones, zeros = jnp.ones((SUB, LANES), F32), jnp.zeros((SUB, LANES), F32)

    ext_ref[0:SUB, :] = branch_ref[rows - SUB :, :]
    ext_ref[SUB : 3 * SUB, :] = jnp.zeros((2 * SUB, LANES), F32)
    ext_ref[SUB : SUB + edge, :] = after_ref[0:edge, :]
    few_ref[...] = jnp.full((SUB, LANES), -1.0, F32)
    near = after_ref[edge : 2 * edge, :]
    few_ref[0:edge, :] = jnp.where(near < 0.0, near, -1.0)
    e_d, e_x, e_p1, e_p2, e_p3, e_p4 = factors(
        *gates_of(ext_ref, SUB, taps_ref, map_ref, param_ref, few_ref[...])
    )

    def line(i, q):
        return all_ref[pl.ds(4 * i + q, SUB, stride=4 * each), :]

    fwd, bwd = (ones, zeros), (ones, zeros)
    for i in range(each):
        k = row * each + i
        fwd = then(fwd, (jnp.where(k < me, line(i, 0), 1.0), jnp.where(k < me, line(i, 1), 0.0)))
        o = each - 1 - i
        k = row * each + o
        bwd = then(
            bwd, (jnp.where(k > me + 1, line(o, 0), 1.0), jnp.where(k > me + 1, line(o, 2), 0.0))
        )
    state_in = prefix_rows(*fwd, False)[1][SUB - 1 : SUB, :]
    beyond = prefix_rows(*bwd, True)[1][0:1, :]
    carry_in = after_ref[3 * edge + 1 : 3 * edge + 2, :] + beyond * after_ref[3 * edge : 3 * edge + 1, :]
    e_gs = zeros
    for t in range(edge - 1, -1, -1):
        gs = after_ref[2 * edge + t : 2 * edge + t + 1, :] + carry_in
        carry_in = e_d[t : t + 1, :] * gs
        e_gs = jnp.where(row == t, gs, e_gs)

    carry = row_of(seg_ref, 2) * carry_in + row_of(seg_ref, 3)
    for i in range(long - 1, -1, -1):
        gs = row_of(g_ref, i) + carry
        carry = own(d_ref, 0, i) * gs
        gm_ref[i * SUB : (i + 1) * SUB, :] = gs
    hidden = row_of(seg_ref, 0) * state_in + row_of(seg_ref, 1)
    for i in range(long):
        gs = row_of(gm_ref, i)
        pre_ref[i * SUB : (i + 1) * SUB, 0:LANES] = gs * (
            hidden * own(p1_ref, 2, i) - own(p2_ref, 3, i)
        )
        pre_ref[i * SUB : (i + 1) * SUB, LANES:] = gs * own(p3_ref, 4, i)
        hidden = own(d_ref, 0, i) * hidden + own(x_ref, 1, i)
        nat_ref[pl.ds(i, SUB, stride=long), :] = rounded(hidden) * row_of(q_ref, i)
    gg_ref[...] = nat_ref[...].astype(BF16)
    last, e_hidden = hidden[SUB - 1 : SUB, :], zeros
    for t in range(edge):
        e_hidden = jnp.where(row == t, last, e_hidden)
        last = e_d[t : t + 1, :] * last + e_x[t : t + 1, :]
    pre_ref[rows : rows + SUB, 0:LANES] = e_gs * (e_hidden * e_p1 - e_p2)
    pre_ref[rows : rows + SUB, LANES:] = e_gs * e_p3
    back = lax.dot_general(
        pre_ref[...].astype(BF16), map_ref[...], (((1,), (1,)), ((), ())), preferred_element_type=F32
    )
    cut = SUB * SUB
    gm_ref[cut:, :] = gm_ref[cut:, :] * p4_ref[cut:, :] + back[cut:rows, :]
    for i in range(SUB):
        gm_ref[i * SUB : (i + 1) * SUB, :] = (
            row_of(gm_ref, i) * own(p4_ref, 5, i) + back[i * SUB : (i + 1) * SUB, :]
        )
    e_gm = e_gs * e_p4 + back[rows:, :]
    turned = [
        jnp.where(row == SUB - 1, e_gm[i : i + 1, :], pltpu.roll(row_of(gm_ref, i), SUB - 1, 0))
        for i in range(edge)
    ]
    for i in range(long):
        total = None
        for j in range(edge + 1):
            k = i + edge - j
            term = taps_ref[j : j + 1, :] * (row_of(gm_ref, k) if k < long else turned[k - long])
            total = term if total is None else total + term
        nat_ref[pl.ds(i, SUB, stride=long), :] = total
    grad_branch = nat_ref[...].astype(BF16)
    gb_ref[...] = grad_branch
    fetch.wait()
    gp_ref[...] = lax.dot_general(
        input_in[...], grad_branch, (((0,), (0,)), ((), ())), preferred_element_type=F32
    ).astype(BF16)


def finish(place, every, after, parts, g, q, patch, seg, branch, taps, a, i, param, block_input):
    rows = g.shape[0]
    return pl.pallas_call(
        finish_kernel,
        in_specs=[pl.BlockSpec(memory_space=pltpu.SMEM)] + [VMEM] * 17 + [pl.BlockSpec(memory_space=pltpu.HBM)],
        out_specs=[VMEM] * 3,
        out_shape=[jax.ShapeDtypeStruct((rows, LANES), BF16)] * 2
        + [jax.ShapeDtypeStruct((block_input.shape[1], LANES), BF16)],
        scratch_shapes=[
            pltpu.VMEM((LANES, 2 * LANES), BF16),
            pltpu.VMEM((rows + SUB, 2 * LANES), F32),
            pltpu.VMEM((rows, LANES), F32),
            pltpu.VMEM((rows, LANES), F32),
            pltpu.VMEM((3 * SUB, LANES), F32),
            pltpu.VMEM((SUB, LANES), F32),
            pltpu.VMEM(block_input.shape, BF16),
            pltpu.SemaphoreType.DMA,
        ],
        cost_estimate=pl.CostEstimate(flops=rows * 600000, bytes_accessed=rows * 8192, transcendentals=0),
        compiler_params=limits(16),
        name="finish",
    )(
        place, every, after, *parts, g, q, patch, seg, branch, taps, a, i, param,
        pltpu.with_memory_space_constraint(block_input, pltpu.HBM),
    )


def partial_kernel(place_ref, gb_ref, gg_ref, wx_ref, wg_ref, keep_ref, send_ref):
    chip, core = place_ref[1], place_ref[2]
    chips, tall = keep_ref.shape[0], keep_ref.shape[1]
    nt = (((1,), (1,)), ((), ()))
    for into, side in ((send_ref, 1 - core), (keep_ref, core)):
        lines = []
        for k in range(chips):
            at = pl.multiple_of(2 * tall * lax.rem(chip + k, chips) + tall * side, 16)
            lines.append(
                jnp.concatenate([gb_ref[pl.ds(at, tall), :], gg_ref[pl.ds(at, tall), :]], axis=1)
            )
        weights = jnp.concatenate([wx_ref[...], wg_ref[...]], axis=1)
        both = lax.dot_general(
            jnp.concatenate(lines, axis=0), weights, nt, preferred_element_type=F32
        ).astype(BF16)
        for k in range(chips):
            into[k] = both[k * tall : (k + 1) * tall]


def partial(place, gb, gg, wx, wg, chips):
    rows, width = gb.shape[0], wx.shape[0]
    shape = jax.ShapeDtypeStruct((chips, rows // (2 * chips), width), BF16)
    return pl.pallas_call(
        partial_kernel,
        in_specs=[pl.BlockSpec(memory_space=pltpu.SMEM)] + [VMEM] * 4,
        out_specs=[VMEM] * 2,
        out_shape=[shape] * 2,
        cost_estimate=pl.CostEstimate(flops=rows * 1000000, bytes_accessed=rows * 8192, transcendentals=0),
        compiler_params=limits(16),
        name="partial",
    )(place, gb, gg, wx, wg)


def shifted(x, axis, by):
    count = lax.axis_size(axis)
    return lax.ppermute(x, axis, [(i, i + by) for i in range(count) if 0 <= i + by < count])


def body(
    block_input, proj_x, proj_gate, conv_taps, gate_a, gate_in, decay_param, log_jump, out_grad
):
    peers = lax.axis_size(SP)
    chips = lax.axis_size("tp_0")
    place = jnp.stack(
        [lax.axis_index(SP), lax.axis_index("tp_0"), lax.axis_index("tp_1")]
    ).astype(jnp.int32)
    param = decay_param.reshape(1, LANES)
    rest = (conv_taps, gate_a, gate_in, param)

    branch, gate, tail = project(block_input, proj_x, proj_gate)
    before = shifted(tail, SP, 1)
    *parts, g, q, misc = local(branch, gate, out_grad, log_jump, *rest)
    sent, head, patch = summary(before, branch, log_jump, *rest, misc, peers)
    every = lax.all_to_all(sent, SP, 0, 0, tiled=True)
    after = shifted(head, SP, -1)
    seg = segments(parts[0], parts[1], g, patch)
    grad_branch, grad_gate, grad_proj = finish(
        place, every, after, parts, g, q, patch, seg, branch, *rest, block_input
    )

    keep, send = partial(place, grad_branch, grad_gate, proj_x, proj_gate, chips)
    got = lax.ppermute(send, "tp_1", [(0, 1), (1, 0)])
    pieces = lax.all_to_all(grad_proj, SP, 0, 0, tiled=True)
    mixed = (keep.astype(F32) + got.astype(F32)).astype(BF16)
    total = mixed[0].astype(F32)
    for by in sorted(range(1, chips), key=lambda k: -min(k, chips - k)):
        arrived = lax.ppermute(mixed[by], "tp_0", [(k, (k + by) % chips) for k in range(chips)])
        total = total + arrived.astype(F32)
    pieces = pieces.reshape(peers, grad_proj.shape[0] // peers, LANES)
    return total.astype(BF16), jnp.sum(pieces.astype(F32), axis=0)


def solution(mesh):
    count = mesh.devices.size
    tp = mesh.shape["tp"]
    sp = count // tp
    first = next(k for k in (8, 4, 2, 1) if sp % k == 0 and sp // k >= k)
    split = Mesh(mesh.devices.reshape(first, sp // first, tp // 2, 2), SP_TP)
    tp_axes = ("tp_0", "tp_1")
    in_specs = (
        P(SP, None),
        P(None, tp_axes),
        P(None, tp_axes),
        P(None, tp_axes),
        P(tp_axes, None, None),
        P(tp_axes, None, None),
        P(tp_axes),
        P(SP, tp_axes),
        P(SP, tp_axes),
    )
    out_specs = (P(SP_TP, None), P(SP, tp_axes))
    return jax.shard_map(body, mesh=split, in_specs=in_specs, out_specs=out_specs, check_vma=False)
```

```python
import jax
import jax.numpy as jnp
from jax import lax
from jax.experimental import pallas as pl
from jax.experimental.pallas import tpu as pltpu
from jax.sharding import Mesh
from jax.sharding import PartitionSpec as P

SP = ("sp_0", "sp_1")
SP_TP = ("sp_0", "sp_1", "tp_0", "tp_1")

GATE_POWER = 8.0
LANES = 128
SUB = 8
F32 = jnp.float32
BF16 = jnp.bfloat16
GELU_A = 0.7978845608028654
GELU_B = 0.044715


VMEM = pl.BlockSpec(memory_space=pltpu.VMEM)


def on_chip(*arrays):
    return [pltpu.with_memory_space_constraint(a, pltpu.VMEM) for a in arrays]


def rounded(x):
    return x.astype(BF16).astype(F32)


def log_sigmoid(x):
    u = jnp.exp(-jnp.abs(x))
    series = u * (1.0 - u * (1 / 2 - u * (1 / 3 - u * (1 / 4 - u * (1 / 5 - u * (1 / 6 - u / 7))))))
    return jnp.minimum(x, 0.0) - jnp.where(u < 0.06, series, jnp.log(1.0 + u))


def one_minus_exp(x):
    near = jnp.maximum(x, -0.5)
    poly = 1.0 + near * (
        1 / 2
        + near
        * (
            1 / 6
            + near
            * (1 / 24 + near * (1 / 120 + near * (1 / 720 + near * (1 / 5040 + near / 40320))))
        )
    )
    return jnp.where(x > -0.5, -near * poly, 1.0 - jnp.exp(x))


def block_diagonal(pair_ref, into_ref, column):
    count, width = pair_ref.shape[0], pair_ref.shape[1]
    for b in range(count):
        at = column + b * width
        into_ref[b * width : (b + 1) * width, at : at + width] = pair_ref[b]


def fill_maps(a_ref, i_ref, map_ref):
    map_ref[...] = jnp.zeros(map_ref.shape, map_ref.dtype)
    block_diagonal(a_ref, map_ref, 0)
    block_diagonal(i_ref, map_ref, LANES)


def gates_of(ext_ref, rows, taps_ref, map_ref, param_ref, log_jump):
    lead = SUB - taps_ref.shape[0] + 1
    total = taps_ref[0:1, :] * ext_ref[lead : lead + rows, :]
    for j in range(1, taps_ref.shape[0]):
        total = total + taps_ref[j : j + 1, :] * ext_ref[lead + j : lead + j + rows, :]
    mixed = total.astype(BF16)
    both = jnp.dot(mixed, map_ref[...], preferred_element_type=F32)
    rec = jax.nn.sigmoid(both[:, :LANES])
    ing = jax.nn.sigmoid(both[:, LANES:])
    log_sig = log_sigmoid(param_ref[...])
    log_decay = GATE_POWER * rec * log_sig + log_jump
    decays = jnp.exp(log_decay)
    room = one_minus_exp(log_decay) * (1.0 + decays)
    return mixed.astype(F32), rec, ing, log_sig, decays, room


def gelu_parts(x):
    return jnp.tanh(GELU_A * (x + GELU_B * x * x * x))


def then(first, second):
    return first[0] * second[0], second[0] * first[1] + second[1]


def prefix_rows(a, f, backward):
    row = lax.broadcasted_iota(jnp.int32, a.shape, 0)
    for by in (1, 2, 4):
        shift = SUB - by if backward else by
        keep = row < SUB - by if backward else row >= by
        pa = jnp.where(keep, pltpu.roll(a, shift, 0), 1.0)
        pf = jnp.where(keep, pltpu.roll(f, shift, 0), 0.0)
        a, f = then((pa, pf), (a, f))
    return a, f


def exclusive_rows(a, f, backward):
    row = lax.broadcasted_iota(jnp.int32, a.shape, 0)
    a, f = prefix_rows(a, f, backward)
    shift = SUB - 1 if backward else 1
    keep = row < SUB - 1 if backward else row >= 1
    return (
        jnp.where(keep, pltpu.roll(a, shift, 0), 1.0),
        jnp.where(keep, pltpu.roll(f, shift, 0), 0.0),
    )


def limits(mib):
    return pltpu.CompilerParams(vmem_limit_bytes=mib * 2**20)


def tail_kernel(x_ref, wx_ref, wg_ref, tail_ref, wx_out, wg_out, x_in, sems):
    tall = x_in.shape[0]
    copies = [
        pltpu.make_async_copy(*pair, sems.at[k])
        for k, pair in enumerate(
            ((wx_ref, wx_out), (x_ref.at[x_ref.shape[0] - tall :, :], x_in), (wg_ref, wg_out))
        )
    ]
    for copy in copies:
        copy.start()
    copies[0].wait()
    copies[1].wait()
    tail_ref[...] = rounded(jnp.dot(x_in[...], wx_out[...], preferred_element_type=F32))[SUB:]
    copies[2].wait()


def tail_of(block_input, proj_x, proj_gate):
    width = block_input.shape[1]
    tall = 2 * SUB
    hbm = pl.BlockSpec(memory_space=pltpu.HBM)
    return pl.pallas_call(
        tail_kernel,
        in_specs=[hbm] * 3,
        out_specs=[VMEM] * 3,
        out_shape=[
            jax.ShapeDtypeStruct((SUB, LANES), F32),
            jax.ShapeDtypeStruct((width, LANES), BF16),
            jax.ShapeDtypeStruct((width, LANES), BF16),
        ],
        scratch_shapes=[pltpu.VMEM((tall, width), BF16), pltpu.SemaphoreType.DMA((3,))],
        cost_estimate=pl.CostEstimate(flops=100000000, bytes_accessed=1000000, transcendentals=0),
        compiler_params=limits(8),
        name="tail",
    )(*(pltpu.with_memory_space_constraint(v, pltpu.HBM) for v in (block_input, proj_x, proj_gate)))


def project_kernel(x_ref, wx_ref, wg_ref, branch_ref, gate_ref):
    both = jnp.concatenate([wx_ref[...], wg_ref[...]], axis=1)
    out = rounded(jnp.dot(x_ref[...], both, preferred_element_type=F32))
    branch_ref[...] = out[:, :LANES]
    gate_ref[...] = out[:, LANES:]


def project(block_input, proj_x, proj_gate):
    rows, width = block_input.shape
    return pl.pallas_call(
        project_kernel,
        in_specs=[VMEM] * 3,
        out_specs=[VMEM] * 2,
        out_shape=[jax.ShapeDtypeStruct((rows, LANES), F32)] * 2,
        cost_estimate=pl.CostEstimate(
            flops=4 * rows * width * LANES, bytes_accessed=4 * width * (rows + LANES), transcendentals=0
        ),
        compiler_params=limits(12),
        name="project",
    )(*on_chip(block_input, proj_x, proj_gate))


def factors(mixed, rec, ing, log_sig, decays, room):
    inverse = lax.rsqrt(room)
    norm = room * inverse
    swing = GATE_POWER * log_sig * rec * (1.0 - rec)
    pull = ing * mixed
    return (
        decays,
        norm * pull,
        decays * swing,
        pull * decays * decays * inverse * swing,
        norm * pull * (1.0 - ing),
        norm * ing,
    )


def row_of(ref, i):
    return ref[i * SUB : (i + 1) * SUB, :]


def sublanes():
    return lax.broadcasted_iota(jnp.int32, (SUB, LANES), 0)


def local_kernel(
    branch_ref, gate_ref, out_grad_ref, jump_ref, taps_ref, a_ref, i_ref, param_ref,
    d_ref, x_ref, p1_ref, p2_ref, p3_ref, p4_ref, g_ref, q_ref, misc_ref, ext_ref, map_ref, *nat_refs,
):
    rows = branch_ref.shape[0]
    long = rows // SUB
    ext_ref[0:SUB, :] = jnp.zeros((SUB, LANES), F32)
    ext_ref[SUB:, :] = branch_ref[...]
    fill_maps(a_ref, i_ref, map_ref)
    values = factors(*gates_of(ext_ref, rows, taps_ref, map_ref, param_ref, jump_ref[...]))
    gate = gate_ref[...]
    t = gelu_parts(gate)
    grad = out_grad_ref[...].astype(F32)
    g = grad * (0.5 * gate * (1.0 + t))
    q = grad * (
        0.5 * (1.0 + t) + 0.5 * gate * (1.0 - t * t) * GELU_A * (1.0 + 3.0 * GELU_B * gate * gate)
    )
    into = (d_ref, x_ref, p1_ref, p2_ref, p3_ref, p4_ref, g_ref, q_ref)
    for value, nat in zip((*values, g, q), nat_refs):
        nat[...] = value
    for nat, ref in zip(nat_refs, into):
        for i in range(long):
            ref[i * SUB : (i + 1) * SUB, :] = nat[pl.ds(i, SUB, stride=long), :]
    row = sublanes()
    ones, zeros = jnp.ones((SUB, LANES), F32), jnp.zeros((SUB, LANES), F32)
    fwd, bwd = (ones, zeros), (ones, zeros)
    for i in range(long):
        a, f = row_of(d_ref, i), row_of(x_ref, i)
        if i < SUB:
            a, f = jnp.where(row == 0, 1.0, a), jnp.where(row == 0, 0.0, f)
        fwd = then(fwd, (a, f))
        o = long - 1 - i
        a = row_of(d_ref, o)
        f = a * row_of(g_ref, o)
        if o < SUB:
            a, f = jnp.where(row == 0, 1.0, a), jnp.where(row == 0, 0.0, f)
        bwd = then(bwd, (a, f))
    fa, ff = prefix_rows(*fwd, False)
    ba, bf = prefix_rows(*bwd, True)
    misc_ref[0:1, :] = fa[SUB - 1 : SUB, :]
    misc_ref[1:2, :] = ff[SUB - 1 : SUB, :]
    misc_ref[2:3, :] = ba[0:1, :]
    misc_ref[3:4, :] = bf[0:1, :]
    misc_ref[4:SUB, :] = jnp.zeros((SUB - 4, LANES), F32)
    misc_ref[SUB:, :] = nat_refs[6][0:SUB, :]


def local(branch, gate, out_grad, jump, taps, a, i, param):
    rows = branch.shape[0]
    return pl.pallas_call(
        local_kernel,
        in_specs=[VMEM] * 8,
        out_specs=[VMEM] * 9,
        out_shape=[jax.ShapeDtypeStruct((rows, LANES), F32)] * 8
        + [jax.ShapeDtypeStruct((2 * SUB, LANES), F32)],
        scratch_shapes=[
            pltpu.VMEM((rows + SUB, LANES), F32),
            pltpu.VMEM((LANES, 2 * LANES), BF16),
        ]
        + [pltpu.VMEM((rows, LANES), F32)] * 8,
        cost_estimate=pl.CostEstimate(flops=rows * 300000, bytes_accessed=rows * 8192, transcendentals=0),
        compiler_params=limits(12),
        name="local",
    )(branch, gate, out_grad, jump, taps, a, i, param)


def summary_kernel(
    before_ref, branch_ref, jump_ref, taps_ref, a_ref, i_ref, param_ref, misc_ref,
    sent_ref, head_ref, patch_ref, ext_ref, map_ref,
):
    edge = taps_ref.shape[0] - 1
    ext_ref[0:SUB, :] = before_ref[...]
    ext_ref[SUB : 2 * SUB, :] = branch_ref[0:SUB, :]
    ext_ref[2 * SUB :, :] = jnp.zeros((SUB, LANES), F32)
    fill_maps(a_ref, i_ref, map_ref)
    values = factors(*gates_of(ext_ref, SUB, taps_ref, map_ref, param_ref, jump_ref[0:SUB, :]))
    for k, value in enumerate(values):
        patch_ref[k * SUB : (k + 1) * SUB, :] = value
    d, x = values[0], values[1]
    g = misc_ref[SUB:, :]
    fa, ff = prefix_rows(d, x, False)
    ba, bf = prefix_rows(d, d * g, True)
    whole = then(
        (fa[SUB - 1 : SUB, :], ff[SUB - 1 : SUB, :]), (misc_ref[0:1, :], misc_ref[1:2, :])
    )
    rest = misc_ref[2:3, :], misc_ref[3:4, :]
    late = then(rest, (ba[edge : edge + 1, :], bf[edge : edge + 1, :]))
    back = then(rest, (ba[0:1, :], bf[0:1, :]))
    head_ref[...] = jnp.zeros(head_ref.shape, F32)
    head_ref[0:edge, :] = branch_ref[0:edge, :]
    head_ref[edge : 2 * edge, :] = jump_ref[0:edge, :]
    head_ref[2 * edge : 3 * edge, :] = misc_ref[SUB : SUB + edge, :]
    head_ref[3 * edge : 3 * edge + 1, :] = late[0]
    head_ref[3 * edge + 1 : 3 * edge + 2, :] = late[1]
    row = sublanes()
    lines = jnp.where(row % 4 == 0, whole[0], jnp.where(row % 4 == 1, whole[1], back[1]))
    for k in range(sent_ref.shape[0] // SUB):
        sent_ref[k * SUB : (k + 1) * SUB, :] = lines


def summary(before, branch, jump, taps, a, i, param, misc, peers):
    return pl.pallas_call(
        summary_kernel,
        in_specs=[VMEM] * 8,
        out_specs=[VMEM] * 3,
        out_shape=[
            jax.ShapeDtypeStruct((peers * 4, LANES), F32),
            jax.ShapeDtypeStruct((2 * SUB, LANES), F32),
            jax.ShapeDtypeStruct((6 * SUB, LANES), F32),
        ],
        scratch_shapes=[
            pltpu.VMEM((3 * SUB, LANES), F32),
            pltpu.VMEM((LANES, 2 * LANES), BF16),
        ],
        cost_estimate=pl.CostEstimate(flops=10000000, bytes_accessed=1000000, transcendentals=0),
        compiler_params=limits(8),
        name="summary",
    )(before, branch, jump, taps, a, i, param, misc)


def patched(ref, patch_ref, k, i, row):
    if i >= SUB:
        return row_of(ref, i)
    at = k * SUB + i
    return jnp.where(row == 0, patch_ref[at : at + 1, :], row_of(ref, i))


def segments_kernel(d_ref, x_ref, g_ref, patch_ref, seg_ref):
    long = d_ref.shape[0] // SUB
    row = sublanes()
    fa, ff = jnp.ones((SUB, LANES), F32), jnp.zeros((SUB, LANES), F32)
    bf = ff
    for i in range(long):
        fa, ff = then((fa, ff), (patched(d_ref, patch_ref, 0, i, row), patched(x_ref, patch_ref, 1, i, row)))
        o = long - 1 - i
        bf = patched(d_ref, patch_ref, 0, o, row) * (row_of(g_ref, o) + bf)
    ea, ef = exclusive_rows(fa, ff, False)
    ra, rf = exclusive_rows(fa, bf, True)
    for k, value in enumerate((ea, ef, ra, rf)):
        seg_ref[k * SUB : (k + 1) * SUB, :] = value


def segments(d, x, g, patch):
    return pl.pallas_call(
        segments_kernel,
        in_specs=[VMEM] * 4,
        out_specs=VMEM,
        out_shape=jax.ShapeDtypeStruct((4 * SUB, LANES), F32),
        cost_estimate=pl.CostEstimate(flops=50000000, bytes_accessed=1000000, transcendentals=0),
        compiler_params=limits(8),
        name="segments",
    )(d, x, g, patch)


def turn_kernel(input_ref, turned_ref, input_in, sems):
    steps = sems.shape[0]
    wide = input_in.shape[1] // steps
    spans = [slice(k * wide, (k + 1) * wide) for k in range(steps)]
    copies = [
        pltpu.make_async_copy(input_ref.at[:, at], input_in.at[:, at], sems.at[k])
        for k, at in enumerate(spans)
    ]
    for copy in copies:
        copy.start()
    for copy, at in zip(copies, spans):
        copy.wait()
        turned_ref[at, :] = input_in[:, at].T


def turn(block_input):
    rows, width = block_input.shape
    steps = 4 if width % (4 * LANES) == 0 else 1
    return pl.pallas_call(
        turn_kernel,
        in_specs=[pl.BlockSpec(memory_space=pltpu.HBM)],
        out_specs=VMEM,
        out_shape=jax.ShapeDtypeStruct((width, rows), BF16),
        scratch_shapes=[pltpu.VMEM((rows, width), BF16), pltpu.SemaphoreType.DMA((steps,))],
        cost_estimate=pl.CostEstimate(flops=100000000, bytes_accessed=4 * rows * width, transcendentals=0),
        compiler_params=limits(12),
        name="turn",
    )(pltpu.with_memory_space_constraint(block_input, pltpu.HBM))


def finish_kernel(
    place_ref, all_ref, after_ref, d_ref, x_ref, p1_ref, p2_ref, p3_ref, p4_ref, g_ref, q_ref, patch_ref, seg_ref,
    tail_ref, taps_ref, a_ref, i_ref, param_ref, turned_ref, wx_ref, wg_ref,
    gb_ref, gg_ref, gp_ref, wx_out, wg_out, map_ref, pre_ref, gm_ref, nat_ref, ext_ref, few_ref, sems,
):
    copies = [
        pltpu.make_async_copy(wx_ref, wx_out, sems.at[0]),
        pltpu.make_async_copy(wg_ref, wg_out, sems.at[1]),
    ]
    for copy in copies:
        copy.start()
    edge = taps_ref.shape[0] - 1
    rows = d_ref.shape[0]
    long = rows // SUB
    me = place_ref[0]
    peers = all_ref.shape[0] // 4
    each = peers // SUB
    row = sublanes()

    def own(ref, k, i):
        return patched(ref, patch_ref, k, i, row)

    fill_maps(a_ref, i_ref, map_ref)
    ones, zeros = jnp.ones((SUB, LANES), F32), jnp.zeros((SUB, LANES), F32)

    ext_ref[0:SUB, :] = tail_ref[...]
    ext_ref[SUB : 3 * SUB, :] = jnp.zeros((2 * SUB, LANES), F32)
    ext_ref[SUB : SUB + edge, :] = after_ref[0:edge, :]
    few_ref[...] = jnp.full((SUB, LANES), -1.0, F32)
    near = after_ref[edge : 2 * edge, :]
    few_ref[0:edge, :] = jnp.where(near < 0.0, near, -1.0)
    e_d, e_x, e_p1, e_p2, e_p3, e_p4 = factors(
        *gates_of(ext_ref, SUB, taps_ref, map_ref, param_ref, few_ref[...])
    )

    def line(i, q):
        return all_ref[pl.ds(4 * i + q, SUB, stride=4 * each), :]

    fwd, bwd = (ones, zeros), (ones, zeros)
    for i in range(each):
        k = row * each + i
        fwd = then(fwd, (jnp.where(k < me, line(i, 0), 1.0), jnp.where(k < me, line(i, 1), 0.0)))
        o = each - 1 - i
        k = row * each + o
        bwd = then(
            bwd, (jnp.where(k > me + 1, line(o, 0), 1.0), jnp.where(k > me + 1, line(o, 2), 0.0))
        )
    state_in = prefix_rows(*fwd, False)[1][SUB - 1 : SUB, :]
    beyond = prefix_rows(*bwd, True)[1][0:1, :]
    carry_in = after_ref[3 * edge + 1 : 3 * edge + 2, :] + beyond * after_ref[3 * edge : 3 * edge + 1, :]
    e_gs = zeros
    for t in range(edge - 1, -1, -1):
        gs = after_ref[2 * edge + t : 2 * edge + t + 1, :] + carry_in
        carry_in = e_d[t : t + 1, :] * gs
        e_gs = jnp.where(row == t, gs, e_gs)

    carry = row_of(seg_ref, 2) * carry_in + row_of(seg_ref, 3)
    for i in range(long - 1, -1, -1):
        gs = row_of(g_ref, i) + carry
        carry = own(d_ref, 0, i) * gs
        gm_ref[i * SUB : (i + 1) * SUB, :] = gs
    hidden = row_of(seg_ref, 0) * state_in + row_of(seg_ref, 1)
    for i in range(long):
        gs = row_of(gm_ref, i)
        pre_ref[i * SUB : (i + 1) * SUB, 0:LANES] = gs * (
            hidden * own(p1_ref, 2, i) - own(p2_ref, 3, i)
        )
        pre_ref[i * SUB : (i + 1) * SUB, LANES:] = gs * own(p3_ref, 4, i)
        hidden = own(d_ref, 0, i) * hidden + own(x_ref, 1, i)
        nat_ref[pl.ds(i, SUB, stride=long), :] = rounded(hidden) * row_of(q_ref, i)
    gg_ref[...] = nat_ref[...].astype(BF16)
    last, e_hidden = hidden[SUB - 1 : SUB, :], zeros
    for t in range(edge):
        e_hidden = jnp.where(row == t, last, e_hidden)
        last = e_d[t : t + 1, :] * last + e_x[t : t + 1, :]
    pre_ref[rows : rows + SUB, 0:LANES] = e_gs * (e_hidden * e_p1 - e_p2)
    pre_ref[rows : rows + SUB, LANES:] = e_gs * e_p3
    back = lax.dot_general(
        pre_ref[...].astype(BF16), map_ref[...], (((1,), (1,)), ((), ())), preferred_element_type=F32
    )
    cut = SUB * SUB
    gm_ref[cut:, :] = gm_ref[cut:, :] * p4_ref[cut:, :] + back[cut:rows, :]
    for i in range(SUB):
        gm_ref[i * SUB : (i + 1) * SUB, :] = (
            row_of(gm_ref, i) * own(p4_ref, 5, i) + back[i * SUB : (i + 1) * SUB, :]
        )
    e_gm = e_gs * e_p4 + back[rows:, :]
    turned = [
        jnp.where(row == SUB - 1, e_gm[i : i + 1, :], pltpu.roll(row_of(gm_ref, i), SUB - 1, 0))
        for i in range(edge)
    ]
    for i in range(long):
        total = None
        for j in range(edge + 1):
            k = i + edge - j
            term = taps_ref[j : j + 1, :] * (row_of(gm_ref, k) if k < long else turned[k - long])
            total = term if total is None else total + term
        nat_ref[pl.ds(i, SUB, stride=long), :] = total
    grad_branch = nat_ref[...].astype(BF16)
    gb_ref[...] = grad_branch
    gp_ref[...] = jnp.dot(turned_ref[...], grad_branch, preferred_element_type=F32).astype(BF16)
    for copy in copies:
        copy.wait()


def finish(place, every, after, parts, g, q, patch, seg, tail, taps, a, i, param, turned, wx, wg):
    rows = g.shape[0]
    return pl.pallas_call(
        finish_kernel,
        in_specs=[pl.BlockSpec(memory_space=pltpu.SMEM)] + [VMEM] * 18 + [pl.BlockSpec(memory_space=pltpu.HBM)] * 2,
        out_specs=[VMEM] * 5,
        out_shape=[jax.ShapeDtypeStruct((rows, LANES), BF16)] * 2
        + [jax.ShapeDtypeStruct((turned.shape[0], LANES), BF16)] * 3,
        scratch_shapes=[
            pltpu.VMEM((LANES, 2 * LANES), BF16),
            pltpu.VMEM((rows + SUB, 2 * LANES), F32),
            pltpu.VMEM((rows, LANES), F32),
            pltpu.VMEM((rows, LANES), F32),
            pltpu.VMEM((3 * SUB, LANES), F32),
            pltpu.VMEM((SUB, LANES), F32),
            pltpu.SemaphoreType.DMA((2,)),
        ],
        cost_estimate=pl.CostEstimate(flops=rows * 600000, bytes_accessed=rows * 8192, transcendentals=0),
        compiler_params=limits(16),
        name="finish",
    )(
        place, every, after, *parts, g, q, patch, seg, tail, taps, a, i, param,
        turned, *(pltpu.with_memory_space_constraint(w, pltpu.HBM) for w in (wx, wg)),
    )


def partial_kernel(place_ref, gb_ref, gg_ref, wx_ref, wg_ref, keep_ref, send_ref):
    chip, core = place_ref[1], place_ref[2]
    chips, tall = keep_ref.shape[0], keep_ref.shape[1]
    nt = (((1,), (1,)), ((), ()))
    for into, side in ((send_ref, 1 - core), (keep_ref, core)):
        lines = []
        for k in range(chips):
            at = pl.multiple_of(2 * tall * lax.rem(chip + k, chips) + tall * side, 16)
            lines.append(
                jnp.concatenate([gb_ref[pl.ds(at, tall), :], gg_ref[pl.ds(at, tall), :]], axis=1)
            )
        weights = jnp.concatenate([wx_ref[...], wg_ref[...]], axis=1)
        both = lax.dot_general(
            jnp.concatenate(lines, axis=0), weights, nt, preferred_element_type=F32
        ).astype(BF16)
        for k in range(chips):
            into[k] = both[k * tall : (k + 1) * tall]


def partial(place, gb, gg, wx, wg, chips):
    rows, width = gb.shape[0], wx.shape[0]
    shape = jax.ShapeDtypeStruct((chips, rows // (2 * chips), width), BF16)
    return pl.pallas_call(
        partial_kernel,
        in_specs=[pl.BlockSpec(memory_space=pltpu.SMEM)] + [VMEM] * 4,
        out_specs=[VMEM] * 2,
        out_shape=[shape] * 2,
        cost_estimate=pl.CostEstimate(flops=rows * 1000000, bytes_accessed=rows * 8192, transcendentals=0),
        compiler_params=limits(16),
        name="partial",
    )(place, gb, gg, wx, wg)


def shifted(x, axis, by):
    count = lax.axis_size(axis)
    return lax.ppermute(x, axis, [(i, i + by) for i in range(count) if 0 <= i + by < count])


def body(
    block_input, proj_x, proj_gate, conv_taps, gate_a, gate_in, decay_param, log_jump, out_grad
):
    peers = lax.axis_size(SP)
    chips = lax.axis_size("tp_0")
    place = jnp.stack(
        [lax.axis_index(SP), lax.axis_index("tp_0"), lax.axis_index("tp_1")]
    ).astype(jnp.int32)
    param = decay_param.reshape(1, LANES)
    rest = (conv_taps, gate_a, gate_in, param)

    tail, near_x, near_gate = tail_of(block_input, proj_x, proj_gate)
    before = shifted(tail, SP, 1)
    branch, gate = project(block_input, near_x, near_gate)
    *parts, g, q, misc = local(branch, gate, out_grad, log_jump, *rest)
    sent, head, patch = summary(before, branch, log_jump, *rest, misc, peers)
    every = lax.all_to_all(sent, SP, 0, 0, tiled=True)
    after = shifted(head, SP, -1)
    seg = segments(parts[0], parts[1], g, patch)
    turned = turn(block_input)
    grad_branch, grad_gate, grad_proj, near_x, near_gate = finish(
        place, every, after, parts, g, q, patch, seg, tail, *rest, turned, proj_x, proj_gate
    )

    keep, send = partial(place, grad_branch, grad_gate, near_x, near_gate, chips)
    got = lax.ppermute(send, "tp_1", [(0, 1), (1, 0)])
    pieces = lax.all_to_all(grad_proj, SP, 0, 0, tiled=True)
    mixed = (keep.astype(F32) + got.astype(F32)).astype(BF16)
    total = mixed[0].astype(F32)
    for by in sorted(range(1, chips), key=lambda k: -min(k, chips - k)):
        arrived = lax.ppermute(mixed[by], "tp_0", [(k, (k + by) % chips) for k in range(chips)])
        total = total + arrived.astype(F32)
    pieces = pieces.reshape(peers, grad_proj.shape[0] // peers, LANES)
    return total.astype(BF16), jnp.sum(pieces.astype(F32), axis=0)


def solution(mesh):
    count = mesh.devices.size
    tp = mesh.shape["tp"]
    sp = count // tp
    first = next(k for k in (8, 4, 2, 1) if sp % k == 0 and sp // k >= k)
    split = Mesh(mesh.devices.reshape(first, sp // first, tp // 2, 2), SP_TP)
    tp_axes = ("tp_0", "tp_1")
    in_specs = (
        P(SP, None),
        P(None, tp_axes),
        P(None, tp_axes),
        P(None, tp_axes),
        P(tp_axes, None, None),
        P(tp_axes, None, None),
        P(tp_axes),
        P(SP, tp_axes),
        P(SP, tp_axes),
    )
    out_specs = (P(SP_TP, None), P(SP, tp_axes))
    return jax.shard_map(body, mesh=split, in_specs=in_specs, out_specs=out_specs, check_vma=False)
```

```python
import jax
import jax.numpy as jnp
from jax import lax
from jax.experimental import pallas as pl
from jax.experimental.pallas import tpu as pltpu
from jax.sharding import Mesh
from jax.sharding import PartitionSpec as P

SP = ("sp_0", "sp_1")
SP_TP = ("sp_0", "sp_1", "tp_0", "tp_1")

GATE_POWER = 8.0
LANES = 128
SUB = 8
F32 = jnp.float32
BF16 = jnp.bfloat16
GELU_A = 0.7978845608028654
GELU_B = 0.044715


VMEM = pl.BlockSpec(memory_space=pltpu.VMEM)


def on_chip(*arrays):
    return [pltpu.with_memory_space_constraint(a, pltpu.VMEM) for a in arrays]


def rounded(x):
    return x.astype(BF16).astype(F32)


def log_sigmoid(x):
    u = jnp.exp(-jnp.abs(x))
    series = u * (1.0 - u * (1 / 2 - u * (1 / 3 - u * (1 / 4 - u * (1 / 5 - u * (1 / 6 - u / 7))))))
    return jnp.minimum(x, 0.0) - jnp.where(u < 0.06, series, jnp.log(1.0 + u))


def one_minus_exp(x):
    near = jnp.maximum(x, -0.5)
    poly = 1.0 + near * (
        1 / 2
        + near
        * (
            1 / 6
            + near
            * (1 / 24 + near * (1 / 120 + near * (1 / 720 + near * (1 / 5040 + near / 40320))))
        )
    )
    return jnp.where(x > -0.5, -near * poly, 1.0 - jnp.exp(x))


def block_diagonal(pair_ref, into_ref, column):
    count, width = pair_ref.shape[0], pair_ref.shape[1]
    for b in range(count):
        at = column + b * width
        into_ref[b * width : (b + 1) * width, at : at + width] = pair_ref[b]


def fill_maps(a_ref, i_ref, map_ref):
    map_ref[...] = jnp.zeros(map_ref.shape, map_ref.dtype)
    block_diagonal(a_ref, map_ref, 0)
    block_diagonal(i_ref, map_ref, LANES)


def gates_of(ext_ref, rows, taps_ref, map_ref, param_ref, log_jump):
    lead = SUB - taps_ref.shape[0] + 1
    total = taps_ref[0:1, :] * ext_ref[lead : lead + rows, :]
    for j in range(1, taps_ref.shape[0]):
        total = total + taps_ref[j : j + 1, :] * ext_ref[lead + j : lead + j + rows, :]
    mixed = total.astype(BF16)
    both = jnp.dot(mixed, map_ref[...], preferred_element_type=F32)
    rec = jax.nn.sigmoid(both[:, :LANES])
    ing = jax.nn.sigmoid(both[:, LANES:])
    log_sig = log_sigmoid(param_ref[...])
    log_decay = GATE_POWER * rec * log_sig + log_jump
    decays = jnp.exp(log_decay)
    room = one_minus_exp(log_decay) * (1.0 + decays)
    return mixed.astype(F32), rec, ing, log_sig, decays, room


def gelu_parts(x):
    return jnp.tanh(GELU_A * (x + GELU_B * x * x * x))


def then(first, second):
    return first[0] * second[0], second[0] * first[1] + second[1]


def prefix_rows(a, f, backward):
    row = lax.broadcasted_iota(jnp.int32, a.shape, 0)
    for by in (1, 2, 4):
        shift = SUB - by if backward else by
        keep = row < SUB - by if backward else row >= by
        pa = jnp.where(keep, pltpu.roll(a, shift, 0), 1.0)
        pf = jnp.where(keep, pltpu.roll(f, shift, 0), 0.0)
        a, f = then((pa, pf), (a, f))
    return a, f


def exclusive_rows(a, f, backward):
    row = lax.broadcasted_iota(jnp.int32, a.shape, 0)
    a, f = prefix_rows(a, f, backward)
    shift = SUB - 1 if backward else 1
    keep = row < SUB - 1 if backward else row >= 1
    return (
        jnp.where(keep, pltpu.roll(a, shift, 0), 1.0),
        jnp.where(keep, pltpu.roll(f, shift, 0), 0.0),
    )


def limits(mib):
    return pltpu.CompilerParams(vmem_limit_bytes=mib * 2**20)


def tail_kernel(x_ref, wx_ref, wg_ref, tail_ref, wx_out, wg_out, x_in, sems):
    tall = x_in.shape[0]
    copies = [
        pltpu.make_async_copy(*pair, sems.at[k])
        for k, pair in enumerate(
            ((wx_ref, wx_out), (x_ref.at[x_ref.shape[0] - tall :, :], x_in), (wg_ref, wg_out))
        )
    ]
    for copy in copies:
        copy.start()
    copies[0].wait()
    copies[1].wait()
    tail_ref[...] = rounded(jnp.dot(x_in[...], wx_out[...], preferred_element_type=F32))[SUB:]
    copies[2].wait()


def tail_of(block_input, proj_x, proj_gate):
    width = block_input.shape[1]
    tall = 2 * SUB
    hbm = pl.BlockSpec(memory_space=pltpu.HBM)
    return pl.pallas_call(
        tail_kernel,
        in_specs=[hbm] * 3,
        out_specs=[VMEM] * 3,
        out_shape=[
            jax.ShapeDtypeStruct((SUB, LANES), F32),
            jax.ShapeDtypeStruct((width, LANES), BF16),
            jax.ShapeDtypeStruct((width, LANES), BF16),
        ],
        scratch_shapes=[pltpu.VMEM((tall, width), BF16), pltpu.SemaphoreType.DMA((3,))],
        cost_estimate=pl.CostEstimate(flops=100000000, bytes_accessed=1000000, transcendentals=0),
        compiler_params=limits(8),
        name="tail",
    )(*(pltpu.with_memory_space_constraint(v, pltpu.HBM) for v in (block_input, proj_x, proj_gate)))


def project_kernel(x_ref, wx_ref, wg_ref, branch_ref, gate_ref):
    both = jnp.concatenate([wx_ref[...], wg_ref[...]], axis=1)
    out = rounded(jnp.dot(x_ref[...], both, preferred_element_type=F32))
    branch_ref[...] = out[:, :LANES]
    gate_ref[...] = out[:, LANES:]


def project(block_input, proj_x, proj_gate):
    rows, width = block_input.shape
    return pl.pallas_call(
        project_kernel,
        in_specs=[VMEM] * 3,
        out_specs=[VMEM] * 2,
        out_shape=[jax.ShapeDtypeStruct((rows, LANES), F32)] * 2,
        cost_estimate=pl.CostEstimate(
            flops=4 * rows * width * LANES, bytes_accessed=4 * width * (rows + LANES), transcendentals=0
        ),
        compiler_params=limits(12),
        name="project",
    )(*on_chip(block_input, proj_x, proj_gate))


def factors(mixed, rec, ing, log_sig, decays, room):
    inverse = lax.rsqrt(room)
    norm = room * inverse
    swing = GATE_POWER * log_sig * rec * (1.0 - rec)
    pull = ing * mixed
    return (
        decays,
        norm * pull,
        decays * swing,
        pull * decays * decays * inverse * swing,
        norm * pull * (1.0 - ing),
        norm * ing,
    )


def row_of(ref, i):
    return ref[i * SUB : (i + 1) * SUB, :]


def sublanes():
    return lax.broadcasted_iota(jnp.int32, (SUB, LANES), 0)


def local_kernel(
    branch_ref, gate_ref, out_grad_ref, jump_ref, taps_ref, a_ref, i_ref, param_ref,
    d_ref, x_ref, p1_ref, p2_ref, p3_ref, p4_ref, g_ref, q_ref, misc_ref, map_ref, ext_ref, *nat_refs,
):
    rows = branch_ref.shape[0]
    long = rows // SUB
    ext_ref[0:SUB, :] = jnp.zeros((SUB, LANES), F32)
    ext_ref[SUB:, :] = branch_ref[...]
    fill_maps(a_ref, i_ref, map_ref)
    values = factors(*gates_of(ext_ref, rows, taps_ref, map_ref, param_ref, jump_ref[...]))
    gate = gate_ref[...]
    t = gelu_parts(gate)
    grad = out_grad_ref[...].astype(F32)
    g = grad * (0.5 * gate * (1.0 + t))
    q = grad * (
        0.5 * (1.0 + t) + 0.5 * gate * (1.0 - t * t) * GELU_A * (1.0 + 3.0 * GELU_B * gate * gate)
    )
    into = (d_ref, x_ref, p1_ref, p2_ref, p3_ref, p4_ref, g_ref, q_ref)
    for value, nat in zip((*values, g, q), nat_refs):
        nat[...] = value
    for nat, ref in zip(nat_refs, into):
        for i in range(long):
            ref[i * SUB : (i + 1) * SUB, :] = nat[pl.ds(i, SUB, stride=long), :]
    row = sublanes()
    ones, zeros = jnp.ones((SUB, LANES), F32), jnp.zeros((SUB, LANES), F32)
    fwd, bwd = (ones, zeros), (ones, zeros)
    for i in range(long):
        a, f = row_of(d_ref, i), row_of(x_ref, i)
        if i < SUB:
            a, f = jnp.where(row == 0, 1.0, a), jnp.where(row == 0, 0.0, f)
        fwd = then(fwd, (a, f))
        o = long - 1 - i
        a = row_of(d_ref, o)
        f = a * row_of(g_ref, o)
        if o < SUB:
            a, f = jnp.where(row == 0, 1.0, a), jnp.where(row == 0, 0.0, f)
        bwd = then(bwd, (a, f))
    fa, ff = prefix_rows(*fwd, False)
    ba, bf = prefix_rows(*bwd, True)
    misc_ref[0:1, :] = fa[SUB - 1 : SUB, :]
    misc_ref[1:2, :] = ff[SUB - 1 : SUB, :]
    misc_ref[2:3, :] = ba[0:1, :]
    misc_ref[3:4, :] = bf[0:1, :]
    misc_ref[4:SUB, :] = jnp.zeros((SUB - 4, LANES), F32)
    misc_ref[SUB:, :] = nat_refs[6][0:SUB, :]


def local(branch, gate, out_grad, jump, taps, a, i, param):
    rows = branch.shape[0]
    return pl.pallas_call(
        local_kernel,
        in_specs=[VMEM] * 8,
        out_specs=[VMEM] * 10,
        out_shape=[jax.ShapeDtypeStruct((rows, LANES), F32)] * 8
        + [
            jax.ShapeDtypeStruct((2 * SUB, LANES), F32),
            jax.ShapeDtypeStruct((LANES, 2 * LANES), BF16),
        ],
        scratch_shapes=[
            pltpu.VMEM((rows + SUB, LANES), F32),
        ]
        + [pltpu.VMEM((rows, LANES), F32)] * 8,
        cost_estimate=pl.CostEstimate(flops=rows * 300000, bytes_accessed=rows * 8192, transcendentals=0),
        compiler_params=limits(12),
        name="local",
    )(branch, gate, out_grad, jump, taps, a, i, param)


def summary_kernel(
    before_ref, branch_ref, jump_ref, taps_ref, param_ref, misc_ref, map_ref,
    sent_ref, head_ref, patch_ref, ext_ref,
):
    edge = taps_ref.shape[0] - 1
    ext_ref[0:SUB, :] = before_ref[...]
    ext_ref[SUB : 2 * SUB, :] = branch_ref[0:SUB, :]
    ext_ref[2 * SUB :, :] = jnp.zeros((SUB, LANES), F32)
    values = factors(*gates_of(ext_ref, SUB, taps_ref, map_ref, param_ref, jump_ref[0:SUB, :]))
    for k, value in enumerate(values):
        patch_ref[k * SUB : (k + 1) * SUB, :] = value
    d, x = values[0], values[1]
    g = misc_ref[SUB:, :]
    fa, ff = prefix_rows(d, x, False)
    ba, bf = prefix_rows(d, d * g, True)
    whole = then(
        (fa[SUB - 1 : SUB, :], ff[SUB - 1 : SUB, :]), (misc_ref[0:1, :], misc_ref[1:2, :])
    )
    rest = misc_ref[2:3, :], misc_ref[3:4, :]
    late = then(rest, (ba[edge : edge + 1, :], bf[edge : edge + 1, :]))
    back = then(rest, (ba[0:1, :], bf[0:1, :]))
    head_ref[...] = jnp.zeros(head_ref.shape, F32)
    head_ref[0:edge, :] = branch_ref[0:edge, :]
    head_ref[edge : 2 * edge, :] = jump_ref[0:edge, :]
    head_ref[2 * edge : 3 * edge, :] = misc_ref[SUB : SUB + edge, :]
    head_ref[3 * edge : 3 * edge + 1, :] = late[0]
    head_ref[3 * edge + 1 : 3 * edge + 2, :] = late[1]
    row = sublanes()
    lines = jnp.where(row % 4 == 0, whole[0], jnp.where(row % 4 == 1, whole[1], back[1]))
    for k in range(sent_ref.shape[0] // SUB):
        sent_ref[k * SUB : (k + 1) * SUB, :] = lines


def summary(before, branch, jump, taps, param, misc, maps, peers):
    return pl.pallas_call(
        summary_kernel,
        in_specs=[VMEM] * 7,
        out_specs=[VMEM] * 3,
        out_shape=[
            jax.ShapeDtypeStruct((peers * 4, LANES), F32),
            jax.ShapeDtypeStruct((2 * SUB, LANES), F32),
            jax.ShapeDtypeStruct((6 * SUB, LANES), F32),
        ],
        scratch_shapes=[
            pltpu.VMEM((3 * SUB, LANES), F32),
        ],
        cost_estimate=pl.CostEstimate(flops=10000000, bytes_accessed=1000000, transcendentals=0),
        compiler_params=limits(8),
        name="summary",
    )(before, branch, jump, taps, param, misc, maps)


def patched(ref, patch_ref, k, i, row):
    if i >= SUB:
        return row_of(ref, i)
    at = k * SUB + i
    return jnp.where(row == 0, patch_ref[at : at + 1, :], row_of(ref, i))


def segments_kernel(d_ref, x_ref, g_ref, patch_ref, seg_ref):
    long = d_ref.shape[0] // SUB
    row = sublanes()
    fa, ff = jnp.ones((SUB, LANES), F32), jnp.zeros((SUB, LANES), F32)
    bf = ff
    for i in range(long):
        fa, ff = then((fa, ff), (patched(d_ref, patch_ref, 0, i, row), patched(x_ref, patch_ref, 1, i, row)))
        o = long - 1 - i
        bf = patched(d_ref, patch_ref, 0, o, row) * (row_of(g_ref, o) + bf)
    ea, ef = exclusive_rows(fa, ff, False)
    ra, rf = exclusive_rows(fa, bf, True)
    for k, value in enumerate((ea, ef, ra, rf)):
        seg_ref[k * SUB : (k + 1) * SUB, :] = value


def segments(d, x, g, patch):
    return pl.pallas_call(
        segments_kernel,
        in_specs=[VMEM] * 4,
        out_specs=VMEM,
        out_shape=jax.ShapeDtypeStruct((4 * SUB, LANES), F32),
        cost_estimate=pl.CostEstimate(flops=50000000, bytes_accessed=1000000, transcendentals=0),
        compiler_params=limits(8),
        name="segments",
    )(d, x, g, patch)


def turn_kernel(input_ref, turned_ref, input_in, sems):
    steps = sems.shape[0]
    wide = input_in.shape[1] // steps
    spans = [slice(k * wide, (k + 1) * wide) for k in range(steps)]
    copies = [
        pltpu.make_async_copy(input_ref.at[:, at], input_in.at[:, at], sems.at[k])
        for k, at in enumerate(spans)
    ]
    for copy in copies:
        copy.start()
    for copy, at in zip(copies, spans):
        copy.wait()
        turned_ref[at, :] = input_in[:, at].T


def turn(block_input):
    rows, width = block_input.shape
    steps = 4 if width % (4 * LANES) == 0 else 1
    return pl.pallas_call(
        turn_kernel,
        in_specs=[pl.BlockSpec(memory_space=pltpu.HBM)],
        out_specs=VMEM,
        out_shape=jax.ShapeDtypeStruct((width, rows), BF16),
        scratch_shapes=[pltpu.VMEM((rows, width), BF16), pltpu.SemaphoreType.DMA((steps,))],
        cost_estimate=pl.CostEstimate(flops=100000000, bytes_accessed=4 * rows * width, transcendentals=0),
        compiler_params=limits(12),
        name="turn",
    )(pltpu.with_memory_space_constraint(block_input, pltpu.HBM))


def finish_kernel(
    place_ref, all_ref, after_ref, d_ref, x_ref, p1_ref, p2_ref, p3_ref, p4_ref, g_ref, q_ref, patch_ref, seg_ref,
    tail_ref, taps_ref, param_ref, map_ref, wx_ref, wg_ref,
    both_ref, w_in, pre_ref, gm_ref, nat_ref, ext_ref, few_ref, sems,
):
    copies = [
        pltpu.make_async_copy(wx_ref, w_in.at[:, 0:LANES], sems.at[0]),
        pltpu.make_async_copy(wg_ref, w_in.at[:, LANES : 2 * LANES], sems.at[1]),
    ]
    for copy in copies:
        copy.start()
    edge = taps_ref.shape[0] - 1
    rows = d_ref.shape[0]
    long = rows // SUB
    me = place_ref[0]
    peers = all_ref.shape[0] // 4
    each = peers // SUB
    row = sublanes()

    def own(ref, k, i):
        return patched(ref, patch_ref, k, i, row)

    ones, zeros = jnp.ones((SUB, LANES), F32), jnp.zeros((SUB, LANES), F32)

    ext_ref[0:SUB, :] = tail_ref[...]
    ext_ref[SUB : 3 * SUB, :] = jnp.zeros((2 * SUB, LANES), F32)
    ext_ref[SUB : SUB + edge, :] = after_ref[0:edge, :]
    few_ref[...] = jnp.full((SUB, LANES), -1.0, F32)
    near = after_ref[edge : 2 * edge, :]
    few_ref[0:edge, :] = jnp.where(near < 0.0, near, -1.0)
    e_d, e_x, e_p1, e_p2, e_p3, e_p4 = factors(
        *gates_of(ext_ref, SUB, taps_ref, map_ref, param_ref, few_ref[...])
    )

    def line(i, q):
        return all_ref[pl.ds(4 * i + q, SUB, stride=4 * each), :]

    fwd, bwd = (ones, zeros), (ones, zeros)
    for i in range(each):
        k = row * each + i
        fwd = then(fwd, (jnp.where(k < me, line(i, 0), 1.0), jnp.where(k < me, line(i, 1), 0.0)))
        o = each - 1 - i
        k = row * each + o
        bwd = then(
            bwd, (jnp.where(k > me + 1, line(o, 0), 1.0), jnp.where(k > me + 1, line(o, 2), 0.0))
        )
    state_in = prefix_rows(*fwd, False)[1][SUB - 1 : SUB, :]
    beyond = prefix_rows(*bwd, True)[1][0:1, :]
    carry_in = after_ref[3 * edge + 1 : 3 * edge + 2, :] + beyond * after_ref[3 * edge : 3 * edge + 1, :]
    e_gs = zeros
    for t in range(edge - 1, -1, -1):
        gs = after_ref[2 * edge + t : 2 * edge + t + 1, :] + carry_in
        carry_in = e_d[t : t + 1, :] * gs
        e_gs = jnp.where(row == t, gs, e_gs)

    carry = row_of(seg_ref, 2) * carry_in + row_of(seg_ref, 3)
    for i in range(long - 1, -1, -1):
        gs = row_of(g_ref, i) + carry
        carry = own(d_ref, 0, i) * gs
        gm_ref[i * SUB : (i + 1) * SUB, :] = gs
    hidden = row_of(seg_ref, 0) * state_in + row_of(seg_ref, 1)
    for i in range(long):
        gs = row_of(gm_ref, i)
        pre_ref[i * SUB : (i + 1) * SUB, 0:LANES] = gs * (
            hidden * own(p1_ref, 2, i) - own(p2_ref, 3, i)
        )
        pre_ref[i * SUB : (i + 1) * SUB, LANES:] = gs * own(p3_ref, 4, i)
        hidden = own(d_ref, 0, i) * hidden + own(x_ref, 1, i)
        nat_ref[pl.ds(i, SUB, stride=long), :] = rounded(hidden) * row_of(q_ref, i)
    both_ref[:, LANES:] = nat_ref[...].astype(BF16)
    last, e_hidden = hidden[SUB - 1 : SUB, :], zeros
    for t in range(edge):
        e_hidden = jnp.where(row == t, last, e_hidden)
        last = e_d[t : t + 1, :] * last + e_x[t : t + 1, :]
    pre_ref[rows : rows + SUB, 0:LANES] = e_gs * (e_hidden * e_p1 - e_p2)
    pre_ref[rows : rows + SUB, LANES:] = e_gs * e_p3
    back = lax.dot_general(
        pre_ref[...].astype(BF16), map_ref[...], (((1,), (1,)), ((), ())), preferred_element_type=F32
    )
    cut = SUB * SUB
    gm_ref[cut:, :] = gm_ref[cut:, :] * p4_ref[cut:, :] + back[cut:rows, :]
    for i in range(SUB):
        gm_ref[i * SUB : (i + 1) * SUB, :] = (
            row_of(gm_ref, i) * own(p4_ref, 5, i) + back[i * SUB : (i + 1) * SUB, :]
        )
    e_gm = e_gs * e_p4 + back[rows:, :]
    turned = [
        jnp.where(row == SUB - 1, e_gm[i : i + 1, :], pltpu.roll(row_of(gm_ref, i), SUB - 1, 0))
        for i in range(edge)
    ]
    for i in range(long):
        total = None
        for j in range(edge + 1):
            k = i + edge - j
            term = taps_ref[j : j + 1, :] * (row_of(gm_ref, k) if k < long else turned[k - long])
            total = term if total is None else total + term
        nat_ref[pl.ds(i, SUB, stride=long), :] = total
    both_ref[:, 0:LANES] = nat_ref[...].astype(BF16)
    for copy in copies:
        copy.wait()


def finish(place, every, after, parts, g, q, patch, seg, tail, taps, param, maps, wx, wg):
    rows, width = g.shape[0], wx.shape[0]
    return pl.pallas_call(
        finish_kernel,
        in_specs=[pl.BlockSpec(memory_space=pltpu.SMEM)] + [VMEM] * 16 + [pl.BlockSpec(memory_space=pltpu.HBM)] * 2,
        out_specs=[VMEM] * 2,
        out_shape=[
            jax.ShapeDtypeStruct((rows, 2 * LANES), BF16),
            jax.ShapeDtypeStruct((width, 2 * LANES), BF16),
        ],
        scratch_shapes=[
            pltpu.VMEM((rows + SUB, 2 * LANES), F32),
            pltpu.VMEM((rows, LANES), F32),
            pltpu.VMEM((rows, LANES), F32),
            pltpu.VMEM((3 * SUB, LANES), F32),
            pltpu.VMEM((SUB, LANES), F32),
            pltpu.SemaphoreType.DMA((2,)),
        ],
        cost_estimate=pl.CostEstimate(flops=rows * 600000, bytes_accessed=rows * 8192, transcendentals=0),
        compiler_params=limits(16),
        name="finish",
    )(
        place, every, after, *parts, g, q, patch, seg, tail, taps, param, maps,
        *(pltpu.with_memory_space_constraint(w, pltpu.HBM) for w in (wx, wg)),
    )


def products_kernel(place_ref, both_ref, turned_ref, w_ref, gp_ref, keep_ref, send_ref, gp_in, sems):
    steps = sems.shape[0]
    copies = []
    deep = gp_in.shape[0] // steps
    for k in range(steps):
        at = slice(k * deep, (k + 1) * deep)
        gp_in[at, :] = jnp.dot(
            turned_ref[at, :], both_ref[:, 0:LANES], preferred_element_type=F32
        ).astype(BF16)
        copies.append(pltpu.make_async_copy(gp_in.at[at, :], gp_ref.at[at, :], sems.at[k]))
        copies[-1].start()
    chip, core = place_ref[1], place_ref[2]
    chips, tall = keep_ref.shape[0], keep_ref.shape[1]
    for into, side in ((send_ref, 1 - core), (keep_ref, core)):
        lines = []
        for k in range(chips):
            at = pl.multiple_of(2 * tall * lax.rem(chip + k, chips) + tall * side, 16)
            lines.append(both_ref[pl.ds(at, tall), :])
        both = lax.dot_general(
            jnp.concatenate(lines, axis=0),
            w_ref[...],
            (((1,), (1,)), ((), ())),
            preferred_element_type=F32,
        ).astype(BF16)
        for k in range(chips):
            into[k] = both[k * tall : (k + 1) * tall]
    for copy in copies:
        copy.wait()


def products(place, both, turned, w, chips):
    rows, width = both.shape[0], turned.shape[0]
    shape = jax.ShapeDtypeStruct((chips, rows // (2 * chips), width), BF16)
    steps = 4 if width % (4 * LANES) == 0 else 1
    return pl.pallas_call(
        products_kernel,
        in_specs=[pl.BlockSpec(memory_space=pltpu.SMEM)] + [VMEM] * 3,
        out_specs=[pl.BlockSpec(memory_space=pltpu.HBM), VMEM, VMEM],
        out_shape=[pltpu.HBM((width, LANES), BF16), shape, shape],
        scratch_shapes=[pltpu.VMEM((width, LANES), BF16), pltpu.SemaphoreType.DMA((steps,))],
        cost_estimate=pl.CostEstimate(flops=rows * 1000000, bytes_accessed=rows * 8192, transcendentals=0),
        compiler_params=limits(16),
        name="products",
    )(place, both, turned, w)


def join_kernel(keep_ref, got_ref, *refs):
    for k, ref in enumerate(refs):
        ref[...] = (keep_ref[k].astype(F32) + got_ref[k].astype(F32)).astype(BF16)


def join(keep, got):
    shape = jax.ShapeDtypeStruct(keep.shape[1:], BF16)
    return pl.pallas_call(
        join_kernel,
        in_specs=[VMEM] * 2,
        out_specs=[VMEM] * keep.shape[0],
        out_shape=[shape] * keep.shape[0],
        cost_estimate=pl.CostEstimate(flops=10000000, bytes_accessed=1000000, transcendentals=0),
        compiler_params=limits(8),
        name="join",
    )(keep, got)


def closing_kernel(pieces_ref, own_ref, *refs):
    *arrived, total_ref, proj_ref = refs
    total = own_ref[...].astype(F32)
    for ref in arrived:
        total = total + ref[...].astype(F32)
    total_ref[...] = total.astype(BF16)
    tall = proj_ref.shape[0]
    proj = pieces_ref[0:tall, :].astype(F32)
    for k in range(1, pieces_ref.shape[0] // tall):
        proj = proj + pieces_ref[k * tall : (k + 1) * tall, :].astype(F32)
    proj_ref[...] = proj


def closing(pieces, own, arrived, tall):
    return pl.pallas_call(
        closing_kernel,
        in_specs=[VMEM] * (2 + len(arrived)),
        out_specs=[VMEM] * 2,
        out_shape=[
            jax.ShapeDtypeStruct(own.shape, BF16),
            jax.ShapeDtypeStruct((tall, LANES), F32),
        ],
        cost_estimate=pl.CostEstimate(flops=10000000, bytes_accessed=1000000, transcendentals=0),
        compiler_params=limits(8),
        name="closing",
    )(pieces, own, *arrived)


def shifted(x, axis, by):
    count = lax.axis_size(axis)
    return lax.ppermute(x, axis, [(i, i + by) for i in range(count) if 0 <= i + by < count])


def body(
    block_input, proj_x, proj_gate, conv_taps, gate_a, gate_in, decay_param, log_jump, out_grad
):
    peers = lax.axis_size(SP)
    chips = lax.axis_size("tp_0")
    place = jnp.stack(
        [lax.axis_index(SP), lax.axis_index("tp_0"), lax.axis_index("tp_1")]
    ).astype(jnp.int32)
    param = decay_param.reshape(1, LANES)
    tail, near_x, near_gate = tail_of(block_input, proj_x, proj_gate)
    before = shifted(tail, SP, 1)
    branch, gate = project(block_input, near_x, near_gate)
    *parts, g, q, misc, maps = local(
        branch, gate, out_grad, log_jump, conv_taps, gate_a, gate_in, param
    )
    sent, head, patch = summary(before, branch, log_jump, conv_taps, param, misc, maps, peers)
    every = lax.all_to_all(sent, SP, 0, 0, tiled=True)
    after = shifted(head, SP, -1)
    seg = segments(parts[0], parts[1], g, patch)
    turned = turn(block_input)
    both, weights = finish(
        place, every, after, parts, g, q, patch, seg, tail, conv_taps, param, maps, proj_x, proj_gate
    )
    grad_proj, keep, send = products(place, both, turned, weights, chips)

    got = lax.ppermute(send, "tp_1", [(0, 1), (1, 0)])
    pieces = lax.all_to_all(grad_proj, SP, 0, 0, tiled=True)
    mixed = join(keep, got)
    arrived = [
        lax.ppermute(mixed[by], "tp_0", [(k, (k + by) % chips) for k in range(chips)])
        for by in sorted(range(1, chips), key=lambda k: -min(k, chips - k))
    ]
    return closing(pieces, mixed[0], arrived, grad_proj.shape[0] // peers)


def solution(mesh):
    count = mesh.devices.size
    tp = mesh.shape["tp"]
    sp = count // tp
    first = next(k for k in (8, 4, 2, 1) if sp % k == 0 and sp // k >= k)
    split = Mesh(mesh.devices.reshape(first, sp // first, tp // 2, 2), SP_TP)
    tp_axes = ("tp_0", "tp_1")
    in_specs = (
        P(SP, None),
        P(None, tp_axes),
        P(None, tp_axes),
        P(None, tp_axes),
        P(tp_axes, None, None),
        P(tp_axes, None, None),
        P(tp_axes),
        P(SP, tp_axes),
        P(SP, tp_axes),
    )
    out_specs = (P(SP_TP, None), P(SP, tp_axes))
    return jax.shard_map(body, mesh=split, in_specs=in_specs, out_specs=out_specs, check_vma=False)
```
